128 devices in a mesh: ep: 128 (over z, y, x, core).
Axes of the slice: x: 4, y: 4, z: 4, core: 2. Of those that a mesh axis runs over, the one named last changes fastest.
Arguments:
- tokens: bfloat16 [2048, 2048], P('ep'), may hold values from -6 to 6
- lengths: int32 [2048], P('ep'), may hold values from 1 to 1024, 1048576 in all
- cache_keys: bfloat16 [2048, 1024, 128], P('ep'), may hold values from -6 to 6
- cache_values: bfloat16 [2048, 1024, 128], P('ep'), may hold values from -6 to 6
- mix_gain: float32 [2048], replicated, may hold values from 0.1 to 1.9
- mix_out_gain: float32 [2048], replicated, may hold values from 0.1 to 1.9
- ffn_gain: float32 [2048], replicated, may hold values from 0.1 to 1.9
- ffn_out_gain: float32 [2048], replicated, may hold values from 0.1 to 1.9
- query_weight: bfloat16 [2048, 2048], P(None, 'ep'), may hold values from -0.125 to 0.125
- key_weight: bfloat16 [2048, 128], replicated, may hold values from -0.125 to 0.125
- value_weight: bfloat16 [2048, 128], replicated, may hold values from -0.125 to 0.125
- head_bias: float32 [32], replicated, may hold values from -8 to -2
- output_weight: bfloat16 [2048, 2048], P(None, 'ep'), may hold values from -0.125 to 0.125
- routes: int32 [2048, 6], P('ep'), may hold values from 0 to 127, all different within a row; in each aligned block of 16 rows (0 to 15, 16 to 31, ...) at most 2 rows name the same one
- route_weights: float32 [2048, 6], P('ep'), may hold values from 0.1 to 1
- expert_gate: bfloat16 [128, 2048, 512], P('ep'), may hold values from -0.125 to 0.125
- expert_up: bfloat16 [128, 2048, 512], P('ep'), may hold values from -0.125 to 0.125
- expert_down: bfloat16 [128, 512, 2048], P('ep'), may hold values from -0.25 to 0.25
- shared_gate: bfloat16 [2048, 512], replicated, may hold values from -0.125 to 0.125
- shared_up: bfloat16 [2048, 512], replicated, may hold values from -0.125 to 0.125
- shared_down: bfloat16 [512, 2048], replicated, may hold values from -0.25 to 0.25
Outputs:
- layer_out: bfloat16 [2048, 2048], P('ep')
- new_keys: bfloat16 [2048, 128], P('ep')
- new_values: bfloat16 [2048, 128], P('ep')
The draws below stay inside these ranges and needn't reach their ends.
Inputs may be any that keep to these rules, and one draw needn't show every extreme that they name: `routes`: each row names 6 different experts. Among the rows of one device no expert is named more than 2 times, a bound that some block reaches in some device's rows. `lengths`: the new token stands at this position; cache entries at this position and after are unused. Some sequence has exactly 1024.
All inputs are finite; a program needn't handle non-finite values. No bound on the sum of `lengths` on one device may be relied on, other than what follows from the above.
Results may differ from the reference program's by a relative error of at most 0.013.
Values may be sent and summed in bfloat16 or wider, within the bound.
No kernel may reach another device: no remote copies, remote signals or barrier semaphores. Data moves between devices by JAX's collectives and lax.ppermute only.
A program may use at most 128 MiB of HBM per device.

```python
import math
import jax
import jax.numpy as jnp
import numpy as np
from jax import lax

D = 2048
HD = 64
H = 32
KV = 2
FF = 512
SFF = 512
TOP_K = 6
SEQ_DEV = 16
LEN = 1024
TOKENS = 2048
EXPERTS = 128
CAP = 2
N_EP = 128


def shard_levels(rng, shape, split, smallest, largest):
    def one(dim, shards_of):
        draws = jax.random.uniform(jax.random.fold_in(jax.random.fold_in(rng, 6), dim), (shards_of,), jnp.float32, smallest / len(split), largest / len(split))
        return jnp.repeat(jnp.exp(draws), shape[dim] // shards_of).reshape((-1,) + (1,) * (len(shape) - dim - 1))

    level = one(*split[0])
    for cut in split[1:]:
        level = level * one(*cut)
    return level


def length_profile(number_of, total, bound, skew):
    weights = [(1 << 20) // math.isqrt(standing ** skew) + 1 for standing in range(2, number_of + 1)]
    spare, given = total - bound - (number_of - 1), [1] * (number_of - 1)
    while spare > 0:
        candidates = [i for i in range(number_of - 1) if given[i] < bound]
        mass, remaining = sum([weights[i] for i in candidates]), spare
        for i in candidates:
            more = min(bound - given[i], max(1, remaining * weights[i] // mass), spare)
            given[i] = given[i] + more
            spare = spare - more
    return np.array([bound] + given)


def ragged_sizes(key, amount, total, limit, slope):
    if amount == 2:
        one = jax.random.randint(key, (), max(1, total - limit), min(limit, total - 1) + 1)
        return jnp.stack([one, total - one])
    tallies = jnp.asarray(length_profile(amount, total, limit, slope), jnp.int32)
    pairs = (amount - 1) // 2
    source_of, taker = tallies[1:1 + 2 * pairs:2], tallies[2:2 + 2 * pairs:2]
    slack = jnp.minimum(source_of - 1, limit - taker)
    moved = jax.random.randint(jax.random.fold_in(key, 1), (pairs,), 0, 1 << 20) % (slack + 1)
    tallies = tallies.at[1:1 + 2 * pairs:2].set(source_of - moved).at[2:2 + 2 * pairs:2].set(taker + moved)
    return tallies[jax.random.permutation(jax.random.fold_in(key, 2), amount)]


def routed_block(rng, own, number, rows, amount, top, reach, lean):
    order = jax.random.permutation(rng, amount)
    heavy_load, ordinary = portions_of(amount, rows * top, reach, lean, True), portions_of(amount, rows * top, reach, lean, False)
    places = jnp.arange(amount)

    def named(tallies, offset_by):
        used = int((tallies > 0).sum())
        fixed = max(1, used // 4)
        shifted = fixed + (places - fixed + offset_by * (used - fixed)) % max(1, amount - fixed)
        return jnp.zeros((amount,), jnp.int32).at[order[jnp.where(places < fixed, places, shifted)]].set(jnp.asarray(tallies, jnp.int32))

    tallies = jnp.where(number % 4 == 0, named(heavy_load, number // 4), named(ordinary, number - number // 4 - 1))
    mixed = jax.random.permutation(jax.random.fold_in(own, 3), amount)
    giver, taker = mixed[0:amount // 2 * 2:2], mixed[1:amount // 2 * 2:2]
    room = jnp.minimum(tallies[giver] - 1, reach - tallies[taker]) // 2
    room = jnp.where((giver == order[0]) | (taker == order[0]) | (tallies[taker] == 0), 0, jnp.maximum(room, 0))
    shifted = jax.random.randint(jax.random.fold_in(own, 4), (amount // 2,), 0, 1 << 20) % (room + 1)
    tallies = tallies.at[giver].add(-shifted).at[taker].add(shifted)
    members = jnp.searchsorted(jnp.cumsum(tallies), jnp.arange(rows * top), side="right").astype(jnp.int32)
    grid = members.reshape(top, rows).T
    grid = grid[jax.random.permutation(jax.random.fold_in(own, 1), rows)]
    offset_by = jax.random.randint(jax.random.fold_in(own, 2), (rows, 1), 0, top)
    return jnp.take_along_axis(grid, (jnp.arange(top)[None, :] + offset_by) % top, axis=1)


def portions_of(amount, total, reach, slope, full):
    portions = [(1 << 20) // math.isqrt(standing ** slope) + 1 for standing in range(1, amount + 1)]
    largest = reach if full else min(reach, max(-(-total // amount), total * portions[0] // sum(portions)))
    least = 1 if total - largest >= amount - 1 else 0
    holding, spare = [largest] + [least] * (amount - 1), total - largest - least * (amount - 1)
    while spare > 0:
        candidates = [i for i in range(1, amount) if holding[i] < largest] or [i for i in range(1, amount) if holding[i] < reach]
        whole, remaining = sum([portions[i] for i in candidates]), spare
        for i in candidates:
            more = min(reach - holding[i], max(1, remaining * portions[i] // whole), spare)
            holding[i] = holding[i] + more
            spare = spare - more
    return np.array(holding)


def noise(rng, dims, scale, bound, shards=(), held_as=jnp.bfloat16):
    values = scale * jax.random.normal(rng, dims, jnp.float32)
    if shards:
        values = values * shard_levels(rng, dims, shards, -0.22, 0.18)
    return jnp.clip(values, -bound, bound).astype(held_as)


def setup_inputs(seed: int = 0) -> dict:
    arg_keys = jax.random.split(jax.random.key(seed), 22)
    tokens = noise(arg_keys[0], (TOKENS, D), 1.0, 6.0, ((0, 128),))
    lengths = ragged_sizes(arg_keys[1], TOKENS, TOKENS * LEN // 2, LEN, 2).astype(jnp.int32)
    cache_keys = noise(arg_keys[2], (TOKENS, LEN, KV * HD), 1.0, 6.0, ((0, 128),))
    cache_values = noise(arg_keys[3], (TOKENS, LEN, KV * HD), 1.0, 6.0, ((0, 128),))
    mix_gain = jnp.clip(1.0 + 0.18 * jax.random.normal(arg_keys[4], (D,), jnp.float32), 0.1, 1.9)
    mix_out_gain = jnp.clip(1.0 + 0.18 * jax.random.normal(arg_keys[5], (D,), jnp.float32), 0.1, 1.9)
    ffn_gain = jnp.clip(1.0 + 0.18 * jax.random.normal(arg_keys[6], (D,), jnp.float32), 0.1, 1.9)
    ffn_out_gain = jnp.clip(1.0 + 0.18 * jax.random.normal(arg_keys[7], (D,), jnp.float32), 0.1, 1.9)
    query_weight = noise(arg_keys[8], (D, D), D ** -0.5, 0.125, ((1, 128),))
    key_weight = noise(arg_keys[9], (D, KV * HD), D ** -0.5, 0.125)
    value_weight = noise(arg_keys[10], (D, KV * HD), D ** -0.5, 0.125)
    head_bias = jnp.clip(jax.random.uniform(arg_keys[11], (H,), jnp.float32, -8.0, -2.0), -8.0, -2.0)
    output_weight = noise(arg_keys[12], (D, D), D ** -0.5, 0.125, ((1, 128),))
    routes_keys = jax.random.split(jax.random.fold_in(arg_keys[13], 1), TOKENS // SEQ_DEV)
    routes_turns = jax.random.permutation(jax.random.fold_in(arg_keys[13], 3), TOKENS // SEQ_DEV)
    routes = jax.vmap(lambda own, number: routed_block(jax.random.fold_in(arg_keys[13], 2), own, number, SEQ_DEV, EXPERTS, TOP_K, CAP, 2))(routes_keys, routes_turns).reshape((TOKENS, TOP_K))
    route_weights = jnp.clip(jnp.exp(math.log(1.0) - 2.3025851 * jax.random.uniform(arg_keys[14], (TOKENS, TOP_K), jnp.float32) ** shard_levels(arg_keys[14], (TOKENS, TOP_K), ((0, 128),), -0.2, 0.2)), 0.1, 1.0)
    expert_gate = noise(arg_keys[15], (EXPERTS, D, FF), D ** -0.5, 0.125, ((0, 128),))
    expert_up = noise(arg_keys[16], (EXPERTS, D, FF), D ** -0.5, 0.125, ((0, 128),))
    expert_down = noise(arg_keys[17], (EXPERTS, FF, D), FF ** -0.5, 0.25, ((0, 128),))
    shared_gate = noise(arg_keys[18], (D, SFF), D ** -0.5, 0.125)
    shared_up = noise(arg_keys[19], (D, SFF), D ** -0.5, 0.125)
    shared_down = noise(arg_keys[20], (SFF, D), SFF ** -0.5, 0.25)
    return dict(tokens=tokens, lengths=lengths, cache_keys=cache_keys, cache_values=cache_values, mix_gain=mix_gain, mix_out_gain=mix_out_gain, ffn_gain=ffn_gain, ffn_out_gain=ffn_out_gain, query_weight=query_weight, key_weight=key_weight, value_weight=value_weight, head_bias=head_bias, output_weight=output_weight, routes=routes, route_weights=route_weights, expert_gate=expert_gate, expert_up=expert_up, expert_down=expert_down, shared_gate=shared_gate, shared_up=shared_up, shared_down=shared_down)


def rms_scale(rows, gain):
    return rows * lax.rsqrt(lax.optimization_barrier(jnp.mean(rows * rows, axis=-1, keepdims=True)) + 1e-06) * gain

def attend_block(items, head_bias):
    queries, keys, values, lens = items
    seqs = queries.shape[0]
    group = H // KV
    q4 = queries.reshape(seqs, KV, group, HD).astype(jnp.float32)
    k4 = keys.reshape(seqs, LEN, KV, HD).astype(jnp.float32)
    v4 = values.reshape(seqs, LEN, KV, HD).astype(jnp.float32)
    scores = jnp.einsum('skgd,slkd->skgl', q4, k4) * HD ** (-0.5)
    scores = scores + head_bias.reshape(KV, group)[None, :, :, None]
    valid = (jnp.arange(LEN)[None, :] < lens[:, None])[:, None, None, :]
    log_beta = jax.nn.log_sigmoid(scores)
    log_keep = jnp.where(valid, log_beta - scores, 0.0)
    after = lax.cumsum(log_keep, axis=3, reverse=True) - log_keep
    weights = jnp.where(valid, jnp.exp(log_beta + after), 0.0).astype(jnp.bfloat16)
    out = jnp.einsum('skgl,slkd->skgd', weights.astype(jnp.float32), v4)
    return out.astype(jnp.bfloat16).reshape(seqs, H * HD)

def reference(tokens, lengths, cache_keys, cache_values, mix_gain, mix_out_gain, ffn_gain, ffn_out_gain, query_weight, key_weight, value_weight, head_bias, output_weight, routes, route_weights, expert_gate, expert_up, expert_down, shared_gate, shared_up, shared_down):
    resid = tokens.astype(jnp.float32)
    normed = rms_scale(resid, mix_gain).astype(jnp.bfloat16)
    new_keys = jnp.dot(normed, key_weight, preferred_element_type=jnp.float32).astype(jnp.bfloat16)
    new_values = jnp.dot(normed, value_weight, preferred_element_type=jnp.float32).astype(jnp.bfloat16)
    queries = jnp.dot(normed, query_weight, preferred_element_type=jnp.float32).astype(jnp.bfloat16)
    blocks = TOKENS // SEQ_DEV
    attended = lax.map(lambda items: attend_block(items, head_bias), (queries.reshape(blocks, SEQ_DEV, D), cache_keys.reshape(blocks, SEQ_DEV, LEN, KV * HD), cache_values.reshape(blocks, SEQ_DEV, LEN, KV * HD), lengths.reshape(blocks, SEQ_DEV)))
    attended = attended.reshape(TOKENS, D)
    mixed = jnp.dot(attended, output_weight, preferred_element_type=jnp.float32).astype(jnp.bfloat16)
    resid1 = resid + rms_scale(mixed.astype(jnp.float32), mix_out_gain)
    ffn_in = rms_scale(resid1, ffn_gain).astype(jnp.bfloat16)
    shared_hidden = (jax.nn.silu(jnp.dot(ffn_in, shared_gate, preferred_element_type=jnp.float32)) * jnp.dot(ffn_in, shared_up, preferred_element_type=jnp.float32)).astype(jnp.bfloat16)
    shared_out = jnp.dot(shared_hidden, shared_down, preferred_element_type=jnp.float32)
    flat = routes.reshape(-1)
    onehot = (flat[:, None] == jnp.arange(EXPERTS)[None, :]).astype(jnp.int32)
    onehot = onehot.reshape(N_EP, SEQ_DEV * TOP_K, EXPERTS)
    rank = lax.optimization_barrier(jnp.sum((jnp.cumsum(onehot, axis=1) - onehot) * onehot, axis=2)).reshape(-1)
    assign = jnp.arange(TOKENS * TOP_K)
    source = assign // (SEQ_DEV * TOP_K)
    row_index = (source * CAP + rank).astype(jnp.int32)
    token_of = (assign // TOP_K).astype(jnp.int32)
    table = jnp.full((EXPERTS, N_EP * CAP), TOKENS, jnp.int32).at[flat, row_index].set(token_of)
    weight_table = jnp.zeros((EXPERTS, N_EP * CAP), jnp.float32).at[flat, row_index].set(route_weights.reshape(-1))
    padded = jnp.concatenate([ffn_in, jnp.zeros((1, D), jnp.bfloat16)], axis=0)

    def one_expert(carry, items):
        ids, wts, w_gate, w_up, w_down = items
        rows = padded[ids]
        hidden = (jax.nn.silu(jnp.dot(rows, w_gate, preferred_element_type=jnp.float32)) * jnp.dot(rows, w_up, preferred_element_type=jnp.float32)).astype(jnp.bfloat16)
        result = jnp.dot(hidden, w_down, preferred_element_type=jnp.float32).astype(jnp.bfloat16)
        return (carry.at[ids].add(result.astype(jnp.float32) * wts[:, None]), None)
    routed, unused = lax.scan(one_expert, jnp.zeros((TOKENS + 1, D), jnp.float32), (table, weight_table, expert_gate, expert_up, expert_down))
    routed = routed[:TOKENS]
    layer_out = (resid1 + rms_scale(routed + shared_out, ffn_out_gain)).astype(jnp.bfloat16)
    return (layer_out, new_keys, new_values)
```

```python
import jax
import jax.numpy as jnp
from jax import lax
from jax.experimental import pallas as pl
from jax.experimental.pallas import tpu as pltpu
from jax.sharding import PartitionSpec as P


D = 2048
HD = 64
H = 32
FF = 512
TOP = 6
SEQ = 16
LEN = 1024
EP = 128
GRP = 4
XS = 2
PLANE = 16
COLS = D // GRP
SHARD = D // EP
CAP = 2
CH = CAP * D // 16
NJ = D // CH
EPS = 1e-06
F32 = jnp.float32
BF16 = jnp.bfloat16

VMEM = pl.BlockSpec(memory_space=pltpu.VMEM)
HBM = pl.BlockSpec(memory_space=pltpu.HBM)
SMEM = pl.BlockSpec(memory_space=pltpu.SMEM)
PARAMS = pltpu.CompilerParams(vmem_limit_bytes=40 * 1024 * 1024)


def rms(rows, gain):
    return rows * lax.rsqrt(jnp.mean(rows * rows, axis=-1, keepdims=True) + EPS) * gain


def iota(shape, dim):
    return lax.broadcasted_iota(jnp.int32, shape, dim)


def dot(a, b):
    return jnp.dot(a, b, preferred_element_type=F32)


def dot_nt(a, b):
    return lax.dot_general(a, b, (((1,), (1,)), ((), ())), preferred_element_type=F32)


def start_columns(own, other, core, full, sems):
    copies = [
        pltpu.make_async_copy(own, full.at[:, core], sems.at[0]),
        pltpu.make_async_copy(other, full.at[:, 1 - core], sems.at[1]),
    ]
    for c in copies:
        c.start()
    return copies


def columns(copies, full):
    for c in copies:
        c.wait()
    return full[...].reshape(COLS, D)


def norm_kernel(t0, t1, t2, t3, gain, wk, wv, rows, nk, nv):
    for i, t in enumerate((t0, t1, t2, t3)):
        rows[i * SEQ : (i + 1) * SEQ] = rms(t[...].astype(F32), gain[...]).astype(BF16)
    mine = rows[:SEQ]
    nk[...] = dot(mine, wk[...]).astype(BF16)
    nv[...] = dot(mine, wv[...]).astype(BF16)


def query_kernel(place, rows, own, other, q0, q1, q2, q3, full, sems):
    copies = start_columns(own, other, place[1], full, sems)
    out = dot_nt(rows[...], columns(copies, full)).astype(BF16)
    for i, q in enumerate((q0, q1, q2, q3)):
        q[...] = out[i * SEQ : (i + 1) * SEQ]


SUB = 4
BLK = 256


def attend_kernel(place, lens, q0, q1, q2, q3, bias, keys, values, out, qf, sel, upper, att):
    step = pl.program_id(0)

    @pl.when(step == 0)
    def _():
        for i, q in enumerate((q0, q1, q2, q3)):
            qf[i] = q[...].astype(F32) * HD ** (-0.5)
        row, col = iota((D, 2 * HD), 0), iota((D, 2 * HD), 1)
        x, plane, k = row >> 9, (row >> 5) & (PLANE - 1), row & 31
        sel[...] = (col == (plane >> 3) * HD + (x & 1) * 32 + k).astype(F32).astype(BF16)
        upper[...] = (iota((BLK, BLK), 0) > iota((BLK, BLK), 1)).astype(F32).astype(BF16)

    own = place[0]
    plane = (iota((H, COLS), 1) >> 5) * 2
    masks = [plane + half == iota((H, COLS), 0) for half in range(2)]
    spread = []
    for u in range(SUB):
        parts = []
        for m in range(GRP):
            row = qf[own ^ m, pl.ds(step * SUB + u, 1), :]
            parts.append(jnp.where(masks[m >> 1], jnp.broadcast_to(row, (H, COLS)), 0.0).astype(BF16))
        spread.append(jnp.concatenate(parts, axis=1))
    placed = dot(jnp.concatenate(spread, axis=0), sel[...]).astype(BF16)
    for u in range(SUB):
        z = dot_nt(placed[u * H : (u + 1) * H], keys[u]) + bias[...]
        n = lens[step * SUB + u]
        valid = iota((H, LEN), 1) < n
        soft = jnp.log(1.0 + jnp.exp(-jnp.abs(z)))
        log_beta = jnp.minimum(z, 0.0) - soft
        log_keep = jnp.where(valid, log_beta - z, 0.0)
        high = log_keep.astype(BF16)
        low = (log_keep - high.astype(F32)).astype(BF16)
        carry = jnp.zeros((H, 1), F32)
        blocks = []
        for b in range(LEN // BLK - 1, -1, -1):
            s = slice(b * BLK, (b + 1) * BLK)
            both = dot(jnp.concatenate([high[:, s], low[:, s]], axis=0), upper[...])
            after = both[:H] + both[H:]
            blocks.append(after + carry)
            carry = carry + after[:, :1] + log_keep[:, s][:, :1]
        after = jnp.concatenate(blocks[::-1], axis=1)
        weights = jnp.where(valid, jnp.exp(log_beta + after), 0.0).astype(BF16)
        att[pl.ds((step * SUB + u) * H, H), :] = dot(weights, values[u])

    @pl.when(step == SEQ // SUB - 1)
    def _():
        left = iota((SEQ, 2 * HD), 1) < HD
        for i in range(H // 2):
            even = att[pl.ds(2 * i, SEQ, stride=H), :]
            odd = att[pl.ds(2 * i + 1, SEQ, stride=H), :]
            if 2 * i < H // 2:
                odd = pltpu.roll(odd, HD, 1)
            else:
                even = pltpu.roll(even, HD, 1)
            out[:, i * 2 * HD : (i + 1) * 2 * HD] = jnp.where(left, even, odd).astype(BF16)


def output_kernel(place, a0, a1, a2, a3, own, other, m0, m1, m2, m3, full, sems):
    copies = start_columns(own, other, place[1], full, sems)
    rows = jnp.concatenate([a[...] for a in (a0, a1, a2, a3)], axis=0)
    out = dot_nt(rows, columns(copies, full)).astype(BF16)
    for i, m in enumerate((m0, m1, m2, m3)):
        m[...] = out[i * SEQ : (i + 1) * SEQ]


def places(routes, weights):
    shape = (EP * CAP, NJ * SEQ)
    row = iota(shape, 0)
    named = jnp.zeros(shape, F32)
    weight = jnp.zeros(shape, F32)
    for k in range(TOP):
        hit = jnp.broadcast_to(routes[k : k + 1, :], shape) == row >> 1
        named = named + hit.astype(F32)
        if weights is not None:
            weight = weight + jnp.where(hit, jnp.broadcast_to(weights[k : k + 1, :], shape), 0.0)
    a, b = iota((NJ * SEQ, NJ * SEQ), 0), iota((NJ * SEQ, NJ * SEQ), 1)
    earlier = (((a >> 4) == (b >> 4)) & (a < b)).astype(F32).astype(BF16)
    rank = dot(named.astype(BF16), earlier)
    here = jnp.where((rank == (row & 1).astype(F32)) & (named > 0.0), 1.0, 0.0)
    return here if weights is None else here * weight


def expand(x):
    block = (iota((NJ, NJ * SEQ), 0) == (iota((NJ, NJ * SEQ), 1) >> 4)).astype(F32)
    return (x[:, None, :] * block[None, :, :]).reshape(EP * CAP * NJ, NJ * SEQ)


def route_kernel(routes, send):
    send[...] = expand(places(routes, None)).astype(BF16)


def mix_kernel(place, m0, m1, m2, m3, tokens, mix_gain, ffn_gain, send, resid1, ffn_in, outgoing, pieces):
    for i, m in enumerate((m0, m1, m2, m3)):
        pieces[i] = m[...]
    own = place[0]
    got = [pieces[own ^ m] for m in range(GRP)]
    n = GRP * 128
    col = iota((n, n), 1)
    source = ((col >> 5) & 3) * 128 + (col >> 7) * 32 + (col & 31)
    order = (iota((n, n), 0) == source).astype(F32).astype(BF16)
    parts = []
    for i in range(COLS // 128):
        block = jnp.concatenate([g[:, i * 128 : (i + 1) * 128] for g in got], axis=1)
        parts.append(dot(block, order))
    mixed = jnp.concatenate(parts, axis=1)
    r1 = tokens[...].astype(F32) + rms(mixed, mix_gain[...])
    resid1[...] = r1
    x = rms(r1, ffn_gain[...]).astype(BF16)
    ffn_in[...] = x
    blocks = jnp.concatenate([x[:, j * CH : (j + 1) * CH] for j in range(NJ)], axis=0)
    outgoing[...] = dot(send[...], blocks).astype(BF16)


def expert_kernel(incoming, gate, up, down, outgoing, rows, result, wg, wu, wd, sems):
    copies = [
        pltpu.make_async_copy(w.at[0], v, sems.at[i])
        for i, (w, v) in enumerate(((gate, wg), (up, wu), (down, wd)))
    ]
    for c in copies:
        c.start()
    n = 256
    a, b = iota((n, n), 0), iota((n, n), 1)
    order = (b == (a & 31) * NJ + (a >> 5)).astype(F32).astype(BF16)
    back = (a == (b & 31) * NJ + (b >> 5)).astype(F32).astype(BF16)
    for g in range(EP * 16 // n):
        block = dot(order, incoming[g * n : (g + 1) * n, :]).astype(BF16)
        for j in range(NJ):
            rows[g * 32 : (g + 1) * 32, j * CH : (j + 1) * CH] = block[j * 32 : (j + 1) * 32]
    x = rows[...]
    copies[0].wait()
    gated = jax.nn.silu(dot(x, wg[...]))
    copies[1].wait()
    hidden = (gated * dot(x, wu[...])).astype(BF16)
    copies[2].wait()
    result[...] = dot(hidden, wd[...]).astype(BF16)
    for g in range(EP * 16 // n):
        block = jnp.concatenate(
            [result[g * 32 : (g + 1) * 32, j * CH : (j + 1) * CH] for j in range(NJ)], axis=0
        )
        outgoing[g * n : (g + 1) * n, :] = dot(back, block).astype(BF16)


def final_kernel(returned, routes, weights, resid1, shared, gain, out):
    scaled = expand(places(routes, weights))
    top = scaled.astype(BF16)
    rest = (scaled - top.astype(F32)).astype(BF16)
    got = returned[...]
    total = dot(top.T, got) + dot(rest.T, got)
    routed = jnp.concatenate([total[j * SEQ : (j + 1) * SEQ] for j in range(NJ)], axis=1)
    out[...] = (resid1[...] + rms(routed + shared[...], gain[...])).astype(BF16)


def call(kernel, ins, outs, smem=0, hbm=0, scratch=()):
    return pl.pallas_call(
        kernel,
        in_specs=[SMEM] * smem + [VMEM] * (ins - smem - hbm) + [HBM] * hbm,
        out_specs=[VMEM] * len(outs),
        out_shape=[jax.ShapeDtypeStruct(s, d) for s, d in outs],
        scratch_shapes=list(scratch),
        compiler_params=PARAMS,
    )


def in_hbm(x):
    return pltpu.with_memory_space_constraint(x, pltpu.HBM)


def swap(x, d):
    return lax.ppermute(x, "ep", [(i, i ^ d) for i in range(EP)])


def share(x):
    return [x] + [swap(x, XS * d) for d in range(1, GRP)]


def trade(parts):
    return [parts[0]] + [swap(parts[d], XS * d) for d in range(1, GRP)]


def copies_kernel(x, *refs):
    for i in range(PLANE):
        refs[-1][i] = x[...]


def gather_columns(weight, after=()):
    mine = weight.T
    line = EP // PLANE
    groups = [[g + line * i for i in range(PLANE)] for g in range(line)]
    copies = pl.pallas_call(
        copies_kernel,
        in_specs=[VMEM] + [pl.BlockSpec(memory_space=pl.ANY)] * len(after),
        out_specs=VMEM,
        out_shape=jax.ShapeDtypeStruct((PLANE, SHARD, D), BF16),
        compiler_params=pltpu.CompilerParams(vmem_limit_bytes=4 * 1024 * 1024),
        name="copies",
    )(mine, *after)
    own = lax.all_to_all(copies, "ep", 0, 0, tiled=True, axis_index_groups=groups)
    return own, swap(own, 1)


def body(
    tokens, lengths, cache_keys, cache_values, mix_gain, mix_out_gain, ffn_gain, ffn_out_gain,
    query_weight, key_weight, value_weight, head_bias, output_weight, routes, route_weights,
    expert_gate, expert_up, expert_down, shared_gate, shared_up, shared_down,
):
    here = lax.axis_index("ep")
    place = jnp.stack([here // XS % GRP, here % 2]).astype(jnp.int32)
    group_tokens = share(tokens)
    own_q, other_q = gather_columns(query_weight)
    route_rows = jnp.tile(routes.T, (1, NJ))
    weight_rows = jnp.tile(route_weights.T, (1, NJ))
    (send,) = call(route_kernel, 1, [((EP * 16, NJ * SEQ), BF16)])(route_rows)
    rows, new_keys, new_values = call(
        norm_kernel, 7, [((GRP * SEQ, D), BF16)] + [((SEQ, 2 * HD), BF16)] * 2
    )(*group_tokens, mix_gain[None], key_weight, value_weight)
    piece = ((SEQ, COLS), BF16)
    load = [pltpu.VMEM((PLANE, 2, SHARD, D), BF16), pltpu.SemaphoreType.DMA((2,))]
    queries = call(
        query_kernel, 4, [piece] * GRP, smem=1, hbm=2, scratch=load
    )(place, rows, in_hbm(own_q), in_hbm(other_q))
    own_o, other_o = gather_columns(output_weight, after=(queries[0],))
    queries = trade(queries)

    whole = lambda *shape: pl.BlockSpec(shape, lambda i: (0,) * len(shape))
    cache_spec = pl.BlockSpec((SUB, LEN, 2 * HD), lambda i: (i, 0, 0))
    attend = pl.pallas_call(
        attend_kernel,
        grid=(SEQ // SUB,),
        in_specs=[SMEM, SMEM] + [whole(SEQ, COLS)] * GRP + [whole(H, 1), cache_spec, cache_spec],
        out_specs=whole(SEQ, D),
        out_shape=jax.ShapeDtypeStruct((SEQ, D), BF16),
        scratch_shapes=[
            pltpu.VMEM((GRP, SEQ, COLS), F32),
            pltpu.VMEM((D, 2 * HD), BF16),
            pltpu.VMEM((BLK, BLK), BF16),
            pltpu.VMEM((SEQ * H, 2 * HD), F32),
        ],
        compiler_params=PARAMS,
        name="attend",
    )
    attended = attend(
        place, lengths, *queries, head_bias[:, None], in_hbm(cache_keys), in_hbm(cache_values)
    )

    mixed = trade(
        call(output_kernel, 7, [piece] * GRP, smem=1, hbm=2, scratch=load)(
            place, *share(attended), in_hbm(own_o), in_hbm(other_o)
        )
    )
    resid1, ffn_in, outgoing = call(
        mix_kernel, 9,
        [((SEQ, D), F32), ((SEQ, D), BF16), ((EP * 16, CH), BF16)],
        smem=1, scratch=[pltpu.VMEM((GRP, SEQ, COLS), BF16)],
    )(place, *mixed, tokens, mix_out_gain[None], ffn_gain[None], send)

    incoming = lax.all_to_all(outgoing.reshape(EP, 16, CH), "ep", 0, 0, tiled=True)
    shared_hidden = (
        jax.nn.silu(dot(ffn_in, shared_gate)) * dot(ffn_in, shared_up)
    ).astype(BF16)
    shared_out = dot(shared_hidden, shared_down)
    (result,) = call(
        expert_kernel, 4, [((EP * 16, CH), BF16)], hbm=3,
        scratch=[
            pltpu.VMEM((EP * CAP, D), BF16),
            pltpu.VMEM((EP * CAP, D), BF16),
            pltpu.VMEM((D, FF), BF16),
            pltpu.VMEM((D, FF), BF16),
            pltpu.VMEM((FF, D), BF16),
            pltpu.SemaphoreType.DMA((3,)),
        ],
    )(incoming.reshape(EP * 16, CH), in_hbm(expert_gate), in_hbm(expert_up), in_hbm(expert_down))
    returned = lax.all_to_all(result.reshape(EP, 16, CH), "ep", 0, 0, tiled=True)
    (layer_out,) = call(final_kernel, 6, [((SEQ, D), BF16)])(
        returned.reshape(EP * 16, CH), route_rows, weight_rows, resid1, shared_out,
        ffn_out_gain[None],
    )
    return (layer_out, new_keys, new_values)


def solution(mesh):
    row, full = P("ep", None), P()
    cube, col = P("ep", None, None), P(None, "ep")
    in_specs = (
        row, P("ep"), cube, cube, full, full, full, full, col, full, full, full, col, row, row,
        cube, cube, cube, full, full, full,
    )

    return jax.shard_map(body, mesh=mesh, in_specs=in_specs, out_specs=(row, row, row), check_vma=False)
```

```python
import jax
import jax.numpy as jnp
from jax import lax
from jax.experimental import pallas as pl
from jax.experimental.pallas import tpu as pltpu
from jax.sharding import PartitionSpec as P


D = 2048
HD = 64
H = 32
FF = 512
TOP = 6
SEQ = 16
LEN = 1024
EP = 128
GRP = 4
XS = 2
PLANE = 16
COLS = D // GRP
SHARD = D // EP
CAP = 2
CH = CAP * D // 16
NJ = D // CH
EPS = 1e-06
F32 = jnp.float32
BF16 = jnp.bfloat16

VMEM = pl.BlockSpec(memory_space=pltpu.VMEM)
HBM = pl.BlockSpec(memory_space=pltpu.HBM)
SMEM = pl.BlockSpec(memory_space=pltpu.SMEM)
PARAMS = pltpu.CompilerParams(vmem_limit_bytes=40 * 1024 * 1024)


def rms(rows, gain):
    return rows * lax.rsqrt(jnp.mean(rows * rows, axis=-1, keepdims=True) + EPS) * gain


def iota(shape, dim):
    return lax.broadcasted_iota(jnp.int32, shape, dim)


def dot(a, b):
    return jnp.dot(a, b, preferred_element_type=F32)


def dot_nt(a, b):
    return lax.dot_general(a, b, (((1,), (1,)), ((), ())), preferred_element_type=F32)


def project(place, rows, own, other, outs):
    for core in range(2):

        @pl.when(place[1] == core)
        def _():
            pair = (own, other) if core == 0 else (other, own)
            weight = jnp.concatenate([pair[c][p] for p in range(PLANE) for c in range(2)], axis=0)
            out = dot_nt(rows, weight).astype(BF16)
            for i, o in enumerate(outs):
                o[...] = out[i * SEQ : (i + 1) * SEQ]


def norm_kernel(t0, t1, t2, t3, gain, wk, wv, rows, nk, nv):
    for i, t in enumerate((t0, t1, t2, t3)):
        rows[i * SEQ : (i + 1) * SEQ] = rms(t[...].astype(F32), gain[...]).astype(BF16)
    mine = rows[:SEQ]
    nk[...] = dot(mine, wk[...]).astype(BF16)
    nv[...] = dot(mine, wv[...]).astype(BF16)


def query_kernel(place, rows, own, other, *outs):
    project(place, rows[...], own, other, outs)


SUB = 8
BLK = 256


def attend_kernel(place, lens, q0, q1, q2, q3, bias, keys, values, out, qf, placed, upper, att):
    step = pl.program_id(0)

    @pl.when(step == 0)
    def _():
        upper[...] = (iota((BLK, BLK), 0) > iota((BLK, BLK), 1)).astype(F32).astype(BF16)
        for i, q in enumerate((q0, q1, q2, q3)):
            qf[i] = q[...].astype(F32) * HD ** (-0.5)
        row, col = iota((COLS, 2 * HD), 0), iota((COLS, 2 * HD), 1)
        plane = iota((H, COLS), 1) >> 5
        spread = [[] for _ in range(SEQ)]
        select = []
        for m in range(GRP):
            target = (row >> 8) * HD + (m & 1) * 32 + (row & 31)
            select.append((col == target).astype(F32).astype(BF16))
            mask = plane * 2 + (m >> 1) == iota((H, COLS), 0)
            part = qf[place[0] ^ m]
            for u in range(SEQ):
                rows = jnp.broadcast_to(part[u : u + 1], (H, COLS))
                spread[u].append(jnp.where(mask, rows, 0.0).astype(BF16))
        spread = jnp.concatenate([jnp.concatenate(p, axis=1) for p in spread], axis=0)
        placed[...] = dot(spread, jnp.concatenate(select, axis=0)).astype(BF16)

    count = LEN // BLK
    first = pl.multiple_of(step * SUB * H, SUB * H)
    valid, beta, keep, stacked = [], [], [], []
    for u in range(SUB):
        z = dot_nt(placed[pl.ds(first + u * H, H), :], keys[u]) + bias[...]
        valid.append(iota((H, LEN), 1) < lens[step * SUB + u])
        soft = jnp.log(1.0 + jnp.exp(-jnp.abs(z)))
        beta.append(jnp.minimum(z, 0.0) - soft)
        keep.append(jnp.where(valid[u], beta[u] - z, 0.0))
        high = keep[u].astype(BF16)
        low = (keep[u] - high.astype(F32)).astype(BF16)
        for b in range(count):
            stacked += [high[:, b * BLK : (b + 1) * BLK], low[:, b * BLK : (b + 1) * BLK]]
    later = dot(jnp.concatenate(stacked, axis=0), upper[...])
    for u in range(SUB):
        carry = jnp.zeros((H, 1), F32)
        blocks = []
        for b in range(count - 1, -1, -1):
            at = (u * count + b) * 2 * H
            after = later[at : at + H] + later[at + H : at + 2 * H]
            blocks.append(after + carry)
            carry = carry + after[:, :1] + keep[u][:, b * BLK : b * BLK + 1]
        after = jnp.concatenate(blocks[::-1], axis=1)
        weights = jnp.where(valid[u], jnp.exp(beta[u] + after), 0.0).astype(BF16)
        att[pl.ds(first + u * H, H), :] = dot(weights, values[u])

    @pl.when(step == SEQ // SUB - 1)
    def _():
        left = iota((SEQ, 2 * HD), 1) < HD
        for i in range(H // 2):
            even = att[pl.ds(2 * i, SEQ, stride=H), :]
            odd = att[pl.ds(2 * i + 1, SEQ, stride=H), :]
            if 2 * i < H // 2:
                odd = pltpu.roll(odd, HD, 1)
            else:
                even = pltpu.roll(even, HD, 1)
            out[:, i * 2 * HD : (i + 1) * 2 * HD] = jnp.where(left, even, odd).astype(BF16)


def output_kernel(place, a0, a1, a2, a3, own, other, *outs):
    rows = jnp.concatenate([a[...] for a in (a0, a1, a2, a3)], axis=0)
    project(place, rows, own, other, outs)


def places(routes, weights):
    shape = (EP * CAP, NJ * SEQ)
    row = iota(shape, 0)
    named = jnp.zeros(shape, F32)
    weight = jnp.zeros(shape, F32)
    for k in range(TOP):
        hit = jnp.broadcast_to(routes[k : k + 1, :], shape) == row >> 1
        named = named + hit.astype(F32)
        if weights is not None:
            weight = weight + jnp.where(hit, jnp.broadcast_to(weights[k : k + 1, :], shape), 0.0)
    a, b = iota((NJ * SEQ, NJ * SEQ), 0), iota((NJ * SEQ, NJ * SEQ), 1)
    earlier = (((a >> 4) == (b >> 4)) & (a < b)).astype(F32).astype(BF16)
    rank = dot(named.astype(BF16), earlier)
    here = jnp.where((rank == (row & 1).astype(F32)) & (named > 0.0), 1.0, 0.0)
    return here if weights is None else here * weight


def expand(x):
    block = (iota((NJ, NJ * SEQ), 0) == (iota((NJ, NJ * SEQ), 1) >> 4)).astype(F32)
    return (x[:, None, :] * block[None, :, :]).reshape(EP * CAP * NJ, NJ * SEQ)


def mix_kernel(place, m0, m1, m2, m3, tokens, mix_gain, ffn_gain, routes, resid1, ffn_in, outgoing, pieces):
    for i, m in enumerate((m0, m1, m2, m3)):
        pieces[i] = m[...]
    own = place[0]
    got = [pieces[own ^ m] for m in range(GRP)]
    n = GRP * 128
    col = iota((n, n), 1)
    source = ((col >> 5) & 3) * 128 + (col >> 7) * 32 + (col & 31)
    order = (iota((n, n), 0) == source).astype(F32).astype(BF16)
    parts = []
    for i in range(COLS // 128):
        block = jnp.concatenate([g[:, i * 128 : (i + 1) * 128] for g in got], axis=1)
        parts.append(dot(block, order))
    mixed = jnp.concatenate(parts, axis=1)
    r1 = tokens[...].astype(F32) + rms(mixed, mix_gain[...])
    resid1[...] = r1
    x = rms(r1, ffn_gain[...]).astype(BF16)
    ffn_in[...] = x
    blocks = jnp.concatenate([x[:, j * CH : (j + 1) * CH] for j in range(NJ)], axis=0)
    send = expand(places(routes, None)).astype(BF16)
    outgoing[...] = dot(send, blocks).astype(BF16)


def expert_kernel(incoming, gate, up, down, outgoing, rows, result, wu, wd, sems):
    copies = [
        pltpu.make_async_copy(w.at[0], v, sems.at[i])
        for i, (w, v) in enumerate(((up, wu), (down, wd)))
    ]
    for c in copies:
        c.start()
    n = 256
    a, b = iota((n, n), 0), iota((n, n), 1)
    order = (b == (a & 31) * NJ + (a >> 5)).astype(F32).astype(BF16)
    back = (a == (b & 31) * NJ + (b >> 5)).astype(F32).astype(BF16)
    for g in range(EP * 16 // n):
        block = dot(order, incoming[g * n : (g + 1) * n, :]).astype(BF16)
        for j in range(NJ):
            rows[g * 32 : (g + 1) * 32, j * CH : (j + 1) * CH] = block[j * 32 : (j + 1) * 32]
    x = rows[...]
    gated = jax.nn.silu(dot(x, gate[0]))
    copies[0].wait()
    hidden = (gated * dot(x, wu[...])).astype(BF16)
    copies[1].wait()
    result[...] = dot(hidden, wd[...]).astype(BF16)
    for g in range(EP * 16 // n):
        block = jnp.concatenate(
            [result[g * 32 : (g + 1) * 32, j * CH : (j + 1) * CH] for j in range(NJ)], axis=0
        )
        outgoing[g * n : (g + 1) * n, :] = dot(back, block).astype(BF16)


def final_kernel(returned, routes, weights, resid1, shared, gain, out):
    scaled = expand(places(routes, weights))
    top = scaled.astype(BF16)
    rest = (scaled - top.astype(F32)).astype(BF16)
    got = returned[...]
    total = dot(top.T, got) + dot(rest.T, got)
    routed = jnp.concatenate([total[j * SEQ : (j + 1) * SEQ] for j in range(NJ)], axis=1)
    out[...] = (resid1[...] + rms(routed + shared[...], gain[...])).astype(BF16)


def call(kernel, ins, outs, smem=0, hbm=0, scratch=()):
    return pl.pallas_call(
        kernel,
        in_specs=[SMEM] * smem + [VMEM] * (ins - smem - hbm) + [HBM] * hbm,
        out_specs=[VMEM] * len(outs),
        out_shape=[jax.ShapeDtypeStruct(s, d) for s, d in outs],
        scratch_shapes=list(scratch),
        compiler_params=PARAMS,
    )


def in_hbm(x):
    return pltpu.with_memory_space_constraint(x, pltpu.HBM)


def swap(x, d):
    return lax.ppermute(x, "ep", [(i, i ^ d) for i in range(EP)])


def share(x):
    return [x] + [swap(x, XS * d) for d in range(1, GRP)]


def trade(parts):
    return [parts[0]] + [swap(parts[d], XS * d) for d in range(1, GRP)]


def copies_kernel(x, out):
    for i in range(PLANE):
        out[i] = x[...]


def gather_columns(weight):
    line = EP // PLANE
    groups = [[g + line * i for i in range(PLANE)] for g in range(line)]
    copies = pl.pallas_call(
        copies_kernel,
        in_specs=[VMEM],
        out_specs=VMEM,
        out_shape=jax.ShapeDtypeStruct((PLANE, SHARD, D), BF16),
        compiler_params=pltpu.CompilerParams(vmem_limit_bytes=4 * 1024 * 1024),
        name="copies",
    )(weight.T)
    own = lax.all_to_all(copies, "ep", 0, 0, tiled=True, axis_index_groups=groups)
    return own, swap(own, 1)


def body(
    tokens, lengths, cache_keys, cache_values, mix_gain, mix_out_gain, ffn_gain, ffn_out_gain,
    query_weight, key_weight, value_weight, head_bias, output_weight, routes, route_weights,
    expert_gate, expert_up, expert_down, shared_gate, shared_up, shared_down,
):
    here = lax.axis_index("ep")
    place = jnp.stack([here // XS % GRP, here % 2]).astype(jnp.int32)
    group_tokens = share(tokens)
    own_q, other_q = gather_columns(query_weight)
    route_rows = jnp.tile(routes.T, (1, NJ))
    weight_rows = jnp.tile(route_weights.T, (1, NJ))
    rows, new_keys, new_values = call(
        norm_kernel, 7, [((GRP * SEQ, D), BF16)] + [((SEQ, 2 * HD), BF16)] * 2
    )(*group_tokens, mix_gain[None], key_weight, value_weight)
    piece = ((SEQ, COLS), BF16)
    queries = call(query_kernel, 4, [piece] * GRP, smem=1)(place, rows, own_q, other_q)
    own_o, other_o = gather_columns(output_weight)
    queries = trade(queries)

    whole = lambda *shape: pl.BlockSpec(shape, lambda i: (0,) * len(shape))
    cache_spec = pl.BlockSpec((SUB, LEN, 2 * HD), lambda i: (i, 0, 0))
    attend = pl.pallas_call(
        attend_kernel,
        grid=(SEQ // SUB,),
        in_specs=[SMEM, SMEM] + [whole(SEQ, COLS)] * GRP + [whole(H, 1), cache_spec, cache_spec],
        out_specs=whole(SEQ, D),
        out_shape=jax.ShapeDtypeStruct((SEQ, D), BF16),
        scratch_shapes=[
            pltpu.VMEM((GRP, SEQ, COLS), F32),
            pltpu.VMEM((SEQ * H, 2 * HD), BF16),
            pltpu.VMEM((BLK, BLK), BF16),
            pltpu.VMEM((SEQ * H, 2 * HD), F32),
        ],
        compiler_params=PARAMS,
        name="attend",
    )
    attended = attend(
        place, lengths, *queries, head_bias[:, None], in_hbm(cache_keys), in_hbm(cache_values)
    )

    mixed = trade(
        call(output_kernel, 7, [piece] * GRP, smem=1)(place, *share(attended), own_o, other_o)
    )
    resid1, ffn_in, outgoing = call(
        mix_kernel, 9,
        [((SEQ, D), F32), ((SEQ, D), BF16), ((EP * 16, CH), BF16)],
        smem=1, scratch=[pltpu.VMEM((GRP, SEQ, COLS), BF16)],
    )(place, *mixed, tokens, mix_out_gain[None], ffn_gain[None], route_rows)

    incoming = lax.all_to_all(outgoing.reshape(EP, 16, CH), "ep", 0, 0, tiled=True)
    shared_hidden = (
        jax.nn.silu(dot(ffn_in, shared_gate)) * dot(ffn_in, shared_up)
    ).astype(BF16)
    shared_out = dot(shared_hidden, shared_down)
    result = pl.pallas_call(
        expert_kernel,
        in_specs=[VMEM, VMEM, HBM, HBM],
        out_specs=VMEM,
        out_shape=jax.ShapeDtypeStruct((EP * 16, CH), BF16),
        scratch_shapes=[
            pltpu.VMEM((EP * CAP, D), BF16),
            pltpu.VMEM((EP * CAP, D), BF16),
            pltpu.VMEM((D, FF), BF16),
            pltpu.VMEM((FF, D), BF16),
            pltpu.SemaphoreType.DMA((2,)),
        ],
        compiler_params=PARAMS,
        name="expert",
    )(incoming.reshape(EP * 16, CH), expert_gate, in_hbm(expert_up), in_hbm(expert_down))
    returned = lax.all_to_all(result.reshape(EP, 16, CH), "ep", 0, 0, tiled=True)
    (layer_out,) = call(final_kernel, 6, [((SEQ, D), BF16)])(
        returned.reshape(EP * 16, CH), route_rows, weight_rows, resid1, shared_out,
        ffn_out_gain[None],
    )
    return (layer_out, new_keys, new_values)


def solution(mesh):
    row, full = P("ep", None), P()
    cube, col = P("ep", None, None), P(None, "ep")
    in_specs = (
        row, P("ep"), cube, cube, full, full, full, full, col, full, full, full, col, row, row,
        cube, cube, cube, full, full, full,
    )

    return jax.shard_map(body, mesh=mesh, in_specs=in_specs, out_specs=(row, row, row), check_vma=False)
```

```python
import jax
import jax.numpy as jnp
from jax import lax
from jax.experimental import pallas as pl
from jax.experimental.pallas import tpu as pltpu
from jax.sharding import PartitionSpec as P


D = 2048
HD = 64
H = 32
FF = 512
TOP = 6
SEQ = 16
LEN = 1024
EP = 128
GRP = 4
XS = 2
PLANE = 16
COLS = D // GRP
SHARD = D // EP
CAP = 2
CH = CAP * D // 16
NJ = D // CH
EPS = 1e-06
F32 = jnp.float32
BF16 = jnp.bfloat16

VMEM = pl.BlockSpec(memory_space=pltpu.VMEM)
HBM = pl.BlockSpec(memory_space=pltpu.HBM)
SMEM = pl.BlockSpec(memory_space=pltpu.SMEM)
PARAMS = pltpu.CompilerParams(vmem_limit_bytes=40 * 1024 * 1024)


def rms(rows, gain):
    return rows * lax.rsqrt(jnp.mean(rows * rows, axis=-1, keepdims=True) + EPS) * gain


def iota(shape, dim):
    return lax.broadcasted_iota(jnp.int32, shape, dim)


def dot(a, b):
    return jnp.dot(a, b, preferred_element_type=F32)


def dot_nt(a, b):
    return lax.dot_general(a, b, (((1,), (1,)), ((), ())), preferred_element_type=F32)


def project(place, rows, own, other, outs):
    for core in range(2):

        @pl.when(place[1] == core)
        def _():
            pair = (own, other) if core == 0 else (other, own)
            weight = jnp.concatenate([pair[c][p] for p in range(PLANE) for c in range(2)], axis=0)
            out = dot_nt(rows, weight).astype(BF16)
            for i, o in enumerate(outs):
                o[...] = out[i * SEQ : (i + 1) * SEQ]


def fetch(sources, targets, sems):
    copies = [pltpu.make_async_copy(s, t, sems.at[i]) for i, (s, t) in enumerate(zip(sources, targets))]
    for c in copies:
        c.start()
    return copies


def norm_kernel(t0, t1, t2, t3, others, gain, rows):
    for i, t in enumerate((t0, t1, t2, t3)):
        rows[i * SEQ : (i + 1) * SEQ] = rms(t[...].astype(F32), gain[...]).astype(BF16)
    rows[GRP * SEQ :] = rms(others[...].astype(F32), gain[...]).astype(BF16)


def query_kernel(rows, own, mine, others):
    weight = jnp.concatenate([own[p] for p in range(PLANE)], axis=0)
    out = dot_nt(rows[...], weight).astype(BF16)
    mine[...] = out[: GRP * SEQ]
    others[...] = out[GRP * SEQ :]


def join_kernel(mine, got, *outs):
    for i, o in enumerate(outs):
        o[...] = jnp.concatenate([mine[i * SEQ : (i + 1) * SEQ], got[i * SEQ : (i + 1) * SEQ]], axis=1)


SUB = 8
BLK = 256


def attend_kernel(place, lens, q0, q1, q2, q3, bias, keys, values, out, qf, placed, upper, att, kbuf, vbuf, sems):
    copies = []
    for g in range(SEQ // SUB):
        part = pl.ds(g * SUB, SUB)
        copies.append(
            [
                pltpu.make_async_copy(keys.at[part], kbuf.at[part], sems.at[0, g]),
                pltpu.make_async_copy(values.at[part], vbuf.at[part], sems.at[1, g]),
            ]
        )
        for c in copies[g]:
            c.start()

    upper[...] = (iota((BLK, BLK), 0) > iota((BLK, BLK), 1)).astype(F32).astype(BF16)
    for i, q in enumerate((q0, q1, q2, q3)):
        qf[i] = q[...].astype(F32) * HD ** (-0.5)
    row, col = iota((COLS, 2 * HD), 0), iota((COLS, 2 * HD), 1)
    plane, shard = (row >> 4) & (PLANE - 1), ((row >> 8) ^ place[1]) * SHARD + (row & 15)
    head = ((iota((H, COLS), 1) >> 4) & (PLANE - 1)) * 2
    spread = [[] for _ in range(SEQ)]
    select = []
    for m in range(GRP):
        target = (plane >> 3) * HD + (m & 1) * 32 + shard
        select.append((col == target).astype(F32).astype(BF16))
        mask = head + (m >> 1) == iota((H, COLS), 0)
        part = qf[place[0] ^ m]
        for u in range(SEQ):
            rows = jnp.broadcast_to(part[u : u + 1], (H, COLS))
            spread[u].append(jnp.where(mask, rows, 0.0).astype(BF16))
    spread = jnp.concatenate([jnp.concatenate(p, axis=1) for p in spread], axis=0)
    placed[...] = dot(spread, jnp.concatenate(select, axis=0)).astype(BF16)

    count = LEN // BLK
    for g in range(SEQ // SUB):
        copies[g][0].wait()
        valid, beta, keep, stacked = [], [], [], []
        for u in range(SUB):
            s = g * SUB + u
            z = dot_nt(placed[s * H : (s + 1) * H], kbuf[s]) + bias[...]
            valid.append(iota((H, LEN), 1) < lens[s])
            soft = jnp.log(1.0 + jnp.exp(-jnp.abs(z)))
            beta.append(jnp.minimum(z, 0.0) - soft)
            keep.append(jnp.where(valid[u], beta[u] - z, 0.0))
            high = keep[u].astype(BF16)
            low = (keep[u] - high.astype(F32)).astype(BF16)
            for b in range(count):
                stacked += [high[:, b * BLK : (b + 1) * BLK], low[:, b * BLK : (b + 1) * BLK]]
        later = dot(jnp.concatenate(stacked, axis=0), upper[...])
        copies[g][1].wait()
        for u in range(SUB):
            s = g * SUB + u
            carry = jnp.zeros((H, 1), F32)
            blocks = []
            for b in range(count - 1, -1, -1):
                at = (u * count + b) * 2 * H
                after = later[at : at + H] + later[at + H : at + 2 * H]
                blocks.append(after + carry)
                carry = carry + after[:, :1] + keep[u][:, b * BLK : b * BLK + 1]
            after = jnp.concatenate(blocks[::-1], axis=1)
            weights = jnp.where(valid[u], jnp.exp(beta[u] + after), 0.0).astype(BF16)
            att[s * H : (s + 1) * H, :] = dot(weights, vbuf[s])

    left = iota((SEQ, 2 * HD), 1) < HD
    for i in range(H // 2):
        even = att[pl.ds(2 * i, SEQ, stride=H), :]
        odd = att[pl.ds(2 * i + 1, SEQ, stride=H), :]
        if 2 * i < H // 2:
            odd = pltpu.roll(odd, HD, 1)
        else:
            even = pltpu.roll(even, HD, 1)
        out[:, i * 2 * HD : (i + 1) * 2 * HD] = jnp.where(left, even, odd).astype(BF16)


def attend(place, lengths, queries, bias, keys, values):
    return pl.pallas_call(
        attend_kernel,
        in_specs=[SMEM, SMEM] + [VMEM] * (GRP + 1) + [HBM, HBM],
        out_specs=VMEM,
        out_shape=jax.ShapeDtypeStruct((SEQ, D), BF16),
        scratch_shapes=[
            pltpu.VMEM((GRP, SEQ, COLS), F32),
            pltpu.VMEM((SEQ * H, 2 * HD), BF16),
            pltpu.VMEM((BLK, BLK), BF16),
            pltpu.VMEM((SEQ * H, 2 * HD), F32),
            pltpu.VMEM((SEQ, LEN, 2 * HD), BF16),
            pltpu.VMEM((SEQ, LEN, 2 * HD), BF16),
            pltpu.SemaphoreType.DMA((2, SEQ // SUB)),
        ],
        compiler_params=PARAMS,
        name="attend",
    )(place, lengths, *queries, bias, in_hbm(keys), in_hbm(values))


def output_kernel(place, a0, a1, a2, a3, own, other, *outs):
    rows = jnp.concatenate([a[...] for a in (a0, a1, a2, a3)], axis=0)
    project(place, rows, own, other, outs)


def places(routes, weights):
    shape = (EP * CAP, NJ * SEQ)
    row = iota(shape, 0)
    named = jnp.zeros(shape, F32)
    weight = jnp.zeros(shape, F32)
    for k in range(TOP):
        hit = jnp.broadcast_to(routes[k : k + 1, :], shape) == row >> 1
        named = named + hit.astype(F32)
        if weights is not None:
            weight = weight + jnp.where(hit, jnp.broadcast_to(weights[k : k + 1, :], shape), 0.0)
    a, b = iota((NJ * SEQ, NJ * SEQ), 0), iota((NJ * SEQ, NJ * SEQ), 1)
    earlier = (((a >> 4) == (b >> 4)) & (a < b)).astype(F32).astype(BF16)
    rank = dot(named.astype(BF16), earlier)
    here = jnp.where((rank == (row & 1).astype(F32)) & (named > 0.0), 1.0, 0.0)
    return here if weights is None else here * weight


def expand(x):
    block = (iota((NJ, NJ * SEQ), 0) == (iota((NJ, NJ * SEQ), 1) >> 4)).astype(F32)
    return (x[:, None, :] * block[None, :, :]).reshape(EP * CAP * NJ, NJ * SEQ)


def mix_kernel(place, m0, m1, m2, m3, tokens, mix_gain, ffn_gain, routes, resid1, ffn_in, outgoing, pieces):
    for i, m in enumerate((m0, m1, m2, m3)):
        pieces[i] = m[...]
    own = place[0]
    got = [pieces[own ^ m] for m in range(GRP)]
    n = GRP * 128
    col = iota((n, n), 1)
    source = ((col >> 5) & 3) * 128 + (col >> 7) * 32 + (col & 31)
    order = (iota((n, n), 0) == source).astype(F32).astype(BF16)
    parts = []
    for i in range(COLS // 128):
        block = jnp.concatenate([g[:, i * 128 : (i + 1) * 128] for g in got], axis=1)
        parts.append(dot(block, order))
    mixed = jnp.concatenate(parts, axis=1)
    r1 = tokens[...].astype(F32) + rms(mixed, mix_gain[...])
    resid1[...] = r1
    x = rms(r1, ffn_gain[...]).astype(BF16)
    ffn_in[...] = x
    blocks = jnp.concatenate([x[:, j * CH : (j + 1) * CH] for j in range(NJ)], axis=0)
    send = expand(places(routes, None)).astype(BF16)
    outgoing[...] = dot(send, blocks).astype(BF16)


def expert_kernel(incoming, gate, up, down, outgoing, rows, result, wu, wd, back_rows, sems):
    copies = [
        pltpu.make_async_copy(w.at[0], v, sems.at[i])
        for i, (w, v) in enumerate(((up, wu), (down, wd)))
    ]
    for c in copies:
        c.start()
    n = 256
    a, b = iota((n, n), 0), iota((n, n), 1)
    order = (b == (a & 31) * NJ + (a >> 5)).astype(F32).astype(BF16)
    back = (a == (b & 31) * NJ + (b >> 5)).astype(F32).astype(BF16)
    for g in range(EP * 16 // n):
        block = dot(order, incoming[g * n : (g + 1) * n, :]).astype(BF16)
        for j in range(NJ):
            rows[g * 32 : (g + 1) * 32, j * CH : (j + 1) * CH] = block[j * 32 : (j + 1) * 32]
    x = rows[...]
    gated = jax.nn.silu(dot(x, gate[0]))
    copies[0].wait()
    hidden = (gated * dot(x, wu[...])).astype(BF16)
    copies[1].wait()
    result[...] = dot(hidden, wd[...]).astype(BF16)
    for g in range(EP * 16 // n):
        block = jnp.concatenate(
            [result[g * 32 : (g + 1) * 32, j * CH : (j + 1) * CH] for j in range(NJ)], axis=0
        )
        span = pl.ds(g * n, n)
        back_rows[span, :] = dot(back, block).astype(BF16)
        out = pltpu.make_async_copy(back_rows.at[span], outgoing.at[span], sems.at[2 + g])
        out.start()
        copies.append(out)
    for c in copies[2:]:
        c.wait()


def shared_kernel(x, tokens, mix_far, *refs):
    far, (out, nk, nv), (gain, wk, wv, gate, up, down, sems) = refs[:5], refs[5:8], refs[8:]
    copies = fetch((mix_far, *far), (gain, wk, wv, gate, up, down), sems)
    for c in copies[:3]:
        c.wait()
    mine = rms(tokens[...].astype(F32), gain[...]).astype(BF16)
    nk[...] = dot(mine, wk[...]).astype(BF16)
    nv[...] = dot(mine, wv[...]).astype(BF16)
    copies[3].wait()
    gated = jax.nn.silu(dot(x[...], gate[...]))
    copies[4].wait()
    hidden = (gated * dot(x[...], up[...])).astype(BF16)
    copies[5].wait()
    out[...] = dot(hidden, down[...])


def final_kernel(returned, routes, weights, resid1, shared, gain, out):
    scaled = expand(places(routes, weights))
    top = scaled.astype(BF16)
    rest = (scaled - top.astype(F32)).astype(BF16)
    got = returned[...]
    total = dot(top.T, got) + dot(rest.T, got)
    routed = jnp.concatenate([total[j * SEQ : (j + 1) * SEQ] for j in range(NJ)], axis=1)
    out[...] = (resid1[...] + rms(routed + shared[...], gain[...])).astype(BF16)


def call(kernel, ins, outs, smem=0, hbm=0, scratch=()):
    return pl.pallas_call(
        kernel,
        in_specs=[SMEM] * smem + [VMEM] * (ins - smem - hbm) + [HBM] * hbm,
        out_specs=[VMEM] * len(outs),
        out_shape=[jax.ShapeDtypeStruct(s, d) for s, d in outs],
        scratch_shapes=list(scratch),
        compiler_params=PARAMS,
    )


def in_hbm(x):
    return pltpu.with_memory_space_constraint(x, pltpu.HBM)


def swap(x, d):
    return lax.ppermute(x, "ep", [(i, i ^ d) for i in range(EP)])


def share(x):
    return [x] + [swap(x, XS * d) for d in range(1, GRP)]


def trade(parts):
    return [parts[0]] + [swap(parts[d], XS * d) for d in range(1, GRP)]


def gather_columns(weight):
    line = EP // PLANE
    groups = [[g + line * i for i in range(PLANE)] for g in range(line)]
    copies = jnp.broadcast_to(weight.T[None], (PLANE, SHARD, D))
    return lax.all_to_all(copies, "ep", 0, 0, tiled=True, axis_index_groups=groups)


def body(
    tokens, lengths, cache_keys, cache_values, mix_gain, mix_out_gain, ffn_gain, ffn_out_gain,
    query_weight, key_weight, value_weight, head_bias, output_weight, routes, route_weights,
    expert_gate, expert_up, expert_down, shared_gate, shared_up, shared_down,
):
    here = lax.axis_index("ep")
    place = jnp.stack([here // XS % GRP, here % 2]).astype(jnp.int32)
    group_tokens = share(tokens)
    own_q = gather_columns(query_weight)
    own_o = gather_columns(output_weight)
    route_rows = jnp.tile(routes.T, (1, NJ))
    weight_rows = jnp.tile(route_weights.T, (1, NJ))
    others = swap(jnp.concatenate(group_tokens, axis=0), 1)
    (rows,) = call(norm_kernel, 6, [((2 * GRP * SEQ, D), BF16)])(
        *group_tokens, others, mix_gain[None]
    )
    piece = ((SEQ, COLS), BF16)
    mine, others = call(query_kernel, 2, [((GRP * SEQ, COLS // 2), BF16)] * 2)(rows, own_q)
    got = swap(others, 1)
    queries = call(join_kernel, 2, [piece] * GRP)(mine, got)
    queries = trade(queries)
    attended = attend(
        place, lengths, queries, head_bias[:, None], cache_keys, cache_values
    )
    other_o = swap(own_o, 1)

    mixed = trade(
        call(output_kernel, 7, [piece] * GRP, smem=1)(place, *share(attended), own_o, other_o)
    )
    resid1, ffn_in, outgoing = call(
        mix_kernel, 9,
        [((SEQ, D), F32), ((SEQ, D), BF16), ((EP * 16, CH), BF16)],
        smem=1, scratch=[pltpu.VMEM((GRP, SEQ, COLS), BF16)],
    )(place, *mixed, tokens, mix_out_gain[None], ffn_gain[None], route_rows)

    incoming = lax.all_to_all(outgoing.reshape(EP, 16, CH), "ep", 0, 0, tiled=True)
    result = pl.pallas_call(
        expert_kernel,
        in_specs=[VMEM, VMEM, HBM, HBM],
        out_specs=HBM,
        out_shape=jax.ShapeDtypeStruct((EP * 16, CH), BF16),
        scratch_shapes=[
            pltpu.VMEM((EP * CAP, D), BF16),
            pltpu.VMEM((EP * CAP, D), BF16),
            pltpu.VMEM((D, FF), BF16),
            pltpu.VMEM((FF, D), BF16),
            pltpu.VMEM((EP * 16, CH), BF16),
            pltpu.SemaphoreType.DMA((10,)),
        ],
        compiler_params=PARAMS,
        name="expert",
    )(incoming.reshape(EP * 16, CH), expert_gate, in_hbm(expert_up), in_hbm(expert_down))
    returned = lax.all_to_all(result.reshape(EP, 16, CH), "ep", 0, 0, tiled=True)
    shared_out, new_keys, new_values = pl.pallas_call(
        shared_kernel,
        in_specs=[VMEM, VMEM] + [HBM] * 6,
        out_specs=[VMEM] * 3,
        out_shape=[jax.ShapeDtypeStruct((SEQ, D), F32)]
        + [jax.ShapeDtypeStruct((SEQ, 2 * HD), BF16)] * 2,
        scratch_shapes=[
            pltpu.VMEM((1, D), F32),
            pltpu.VMEM((D, 2 * HD), BF16),
            pltpu.VMEM((D, 2 * HD), BF16),
            pltpu.VMEM((D, FF), BF16),
            pltpu.VMEM((D, FF), BF16),
            pltpu.VMEM((FF, D), BF16),
            pltpu.SemaphoreType.DMA((6,)),
        ],
        compiler_params=PARAMS,
        name="shared",
    )(
        ffn_in, tokens, in_hbm(mix_gain[None]), in_hbm(key_weight), in_hbm(value_weight),
        in_hbm(shared_gate), in_hbm(shared_up), in_hbm(shared_down),
    )
    (layer_out,) = call(final_kernel, 6, [((SEQ, D), BF16)])(
        returned.reshape(EP * 16, CH), route_rows, weight_rows, resid1, shared_out,
        ffn_out_gain[None],
    )
    return (layer_out, new_keys, new_values)


def solution(mesh):
    row, full = P("ep", None), P()
    cube, col = P("ep", None, None), P(None, "ep")
    in_specs = (
        row, P("ep"), cube, cube, full, full, full, full, col, full, full, full, col, row, row,
        cube, cube, cube, full, full, full,
    )

    return jax.shard_map(body, mesh=mesh, in_specs=in_specs, out_specs=(row, row, row), check_vma=False)
```

```python
import jax
import jax.numpy as jnp
from jax import lax
from jax.experimental import pallas as pl
from jax.experimental.pallas import tpu as pltpu
from jax.sharding import PartitionSpec as P


D = 2048
HD = 64
H = 32
FF = 512
TOP = 6
SEQ = 16
LEN = 1024
EP = 128
GRP = 4
XS = 2
PLANE = 16
COLS = D // GRP
SHARD = D // EP
CAP = 2
CH = CAP * D // 16
NJ = D // CH
EPS = 1e-06
F32 = jnp.float32
BF16 = jnp.bfloat16

VMEM = pl.BlockSpec(memory_space=pltpu.VMEM)
HBM = pl.BlockSpec(memory_space=pltpu.HBM)
SMEM = pl.BlockSpec(memory_space=pltpu.SMEM)
PARAMS = pltpu.CompilerParams(vmem_limit_bytes=40 * 1024 * 1024)


def rms(rows, gain):
    return rows * lax.rsqrt(jnp.mean(rows * rows, axis=-1, keepdims=True) + EPS) * gain


def iota(shape, dim):
    return lax.broadcasted_iota(jnp.int32, shape, dim)


def dot(a, b):
    return jnp.dot(a, b, preferred_element_type=F32)


def dot_nt(a, b):
    return lax.dot_general(a, b, (((1,), (1,)), ((), ())), preferred_element_type=F32)


def project(place, rows, own, other, outs):
    for core in range(2):

        @pl.when(place[1] == core)
        def _():
            pair = (own, other) if core == 0 else (other, own)
            weight = jnp.concatenate([pair[c][p] for p in range(PLANE) for c in range(2)], axis=0)
            out = dot_nt(rows, weight).astype(BF16)
            for i, o in enumerate(outs):
                o[...] = out[i * SEQ : (i + 1) * SEQ]


def fetch(sources, targets, sems):
    copies = [pltpu.make_async_copy(s, t, sems.at[i]) for i, (s, t) in enumerate(zip(sources, targets))]
    for c in copies:
        c.start()
    return copies


def norm_kernel(t0, t1, t2, t3, others, gain, rows):
    for i, t in enumerate((t0, t1, t2, t3)):
        rows[i * SEQ : (i + 1) * SEQ] = rms(t[...].astype(F32), gain[...]).astype(BF16)
    rows[GRP * SEQ :] = rms(others[...].astype(F32), gain[...]).astype(BF16)


def query_kernel(rows, own, mine, others):
    weight = jnp.concatenate([own[p] for p in range(PLANE)], axis=0)
    out = dot_nt(rows[...], weight).astype(BF16)
    mine[...] = out[: GRP * SEQ]
    others[...] = out[GRP * SEQ :]


def join_kernel(mine, got, *outs):
    for i, o in enumerate(outs):
        o[...] = jnp.concatenate([mine[i * SEQ : (i + 1) * SEQ], got[i * SEQ : (i + 1) * SEQ]], axis=1)


SUB = 8
BLK = 256


def attend_kernel(place, lens, q0, q1, q2, q3, bias, keys, values, out, qf, placed, upper, att, kbuf, vbuf, sems):
    copies = []
    for g in range(SEQ // SUB):
        part = pl.ds(g * SUB, SUB)
        copies.append(
            [
                pltpu.make_async_copy(keys.at[part], kbuf.at[part], sems.at[0, g]),
                pltpu.make_async_copy(values.at[part], vbuf.at[part], sems.at[1, g]),
            ]
        )
    for c in copies[0]:
        c.start()

    upper[...] = (iota((BLK, BLK), 0) > iota((BLK, BLK), 1)).astype(F32).astype(BF16)
    for i, q in enumerate((q0, q1, q2, q3)):
        qf[i] = q[...].astype(F32) * HD ** (-0.5)
    row, col = iota((COLS, 2 * HD), 0), iota((COLS, 2 * HD), 1)
    plane, shard = (row >> 4) & (PLANE - 1), ((row >> 8) ^ place[1]) * SHARD + (row & 15)
    head = ((iota((H, COLS), 1) >> 4) & (PLANE - 1)) * 2
    spread = [[] for _ in range(SEQ)]
    select = []
    for m in range(GRP):
        target = (plane >> 3) * HD + (m & 1) * 32 + shard
        select.append((col == target).astype(F32).astype(BF16))
        mask = head + (m >> 1) == iota((H, COLS), 0)
        part = qf[place[0] ^ m]
        for u in range(SEQ):
            rows = jnp.broadcast_to(part[u : u + 1], (H, COLS))
            spread[u].append(jnp.where(mask, rows, 0.0).astype(BF16))
    spread = jnp.concatenate([jnp.concatenate(p, axis=1) for p in spread], axis=0)
    placed[...] = dot(spread, jnp.concatenate(select, axis=0)).astype(BF16)

    count = LEN // BLK
    for g in range(SEQ // SUB):
        copies[g][0].wait()
        for c in copies[g + 1] if g + 1 < SEQ // SUB else ():
            c.start()
        valid, beta, keep, stacked = [], [], [], []
        for u in range(SUB):
            s = g * SUB + u
            z = dot_nt(placed[s * H : (s + 1) * H], kbuf[s]) + bias[...]
            valid.append(iota((H, LEN), 1) < lens[s])
            soft = jnp.log(1.0 + jnp.exp(-jnp.abs(z)))
            beta.append(jnp.minimum(z, 0.0) - soft)
            keep.append(jnp.where(valid[u], beta[u] - z, 0.0))
            high = keep[u].astype(BF16)
            low = (keep[u] - high.astype(F32)).astype(BF16)
            for b in range(count):
                stacked += [high[:, b * BLK : (b + 1) * BLK], low[:, b * BLK : (b + 1) * BLK]]
        later = dot(jnp.concatenate(stacked, axis=0), upper[...])
        copies[g][1].wait()
        for u in range(SUB):
            s = g * SUB + u
            carry = jnp.zeros((H, 1), F32)
            blocks = []
            for b in range(count - 1, -1, -1):
                at = (u * count + b) * 2 * H
                after = later[at : at + H] + later[at + H : at + 2 * H]
                blocks.append(after + carry)
                carry = carry + after[:, :1] + keep[u][:, b * BLK : b * BLK + 1]
            after = jnp.concatenate(blocks[::-1], axis=1)
            weights = jnp.where(valid[u], jnp.exp(beta[u] + after), 0.0).astype(BF16)
            att[s * H : (s + 1) * H, :] = dot(weights, vbuf[s])

    left = iota((SEQ, 2 * HD), 1) < HD
    for i in range(H // 2):
        even = att[pl.ds(2 * i, SEQ, stride=H), :]
        odd = att[pl.ds(2 * i + 1, SEQ, stride=H), :]
        if 2 * i < H // 2:
            odd = pltpu.roll(odd, HD, 1)
        else:
            even = pltpu.roll(even, HD, 1)
        out[:, i * 2 * HD : (i + 1) * 2 * HD] = jnp.where(left, even, odd).astype(BF16)


def attend(place, lengths, queries, bias, keys, values):
    return pl.pallas_call(
        attend_kernel,
        in_specs=[SMEM, SMEM] + [VMEM] * (GRP + 1) + [HBM, HBM],
        out_specs=VMEM,
        out_shape=jax.ShapeDtypeStruct((SEQ, D), BF16),
        scratch_shapes=[
            pltpu.VMEM((GRP, SEQ, COLS), F32),
            pltpu.VMEM((SEQ * H, 2 * HD), BF16),
            pltpu.VMEM((BLK, BLK), BF16),
            pltpu.VMEM((SEQ * H, 2 * HD), F32),
            pltpu.VMEM((SEQ, LEN, 2 * HD), BF16),
            pltpu.VMEM((SEQ, LEN, 2 * HD), BF16),
            pltpu.SemaphoreType.DMA((2, SEQ // SUB)),
        ],
        compiler_params=PARAMS,
        name="attend",
    )(place, lengths, *queries, bias, in_hbm(keys), in_hbm(values))


def output_kernel(place, a0, a1, a2, a3, own, other, *outs):
    rows = jnp.concatenate([a[...] for a in (a0, a1, a2, a3)], axis=0)
    project(place, rows, own, other, outs)


def places(routes, weights):
    shape = (EP * CAP, NJ * SEQ)
    row = iota(shape, 0)
    named = jnp.zeros(shape, F32)
    weight = jnp.zeros(shape, F32)
    for k in range(TOP):
        hit = jnp.broadcast_to(routes[k : k + 1, :], shape) == row >> 1
        named = named + hit.astype(F32)
        if weights is not None:
            weight = weight + jnp.where(hit, jnp.broadcast_to(weights[k : k + 1, :], shape), 0.0)
    a, b = iota((NJ * SEQ, NJ * SEQ), 0), iota((NJ * SEQ, NJ * SEQ), 1)
    earlier = (((a >> 4) == (b >> 4)) & (a < b)).astype(F32).astype(BF16)
    rank = dot(named.astype(BF16), earlier)
    here = jnp.where((rank == (row & 1).astype(F32)) & (named > 0.0), 1.0, 0.0)
    return here if weights is None else here * weight


def expand(x):
    block = (iota((NJ, NJ * SEQ), 0) == (iota((NJ, NJ * SEQ), 1) >> 4)).astype(F32)
    return (x[:, None, :] * block[None, :, :]).reshape(EP * CAP * NJ, NJ * SEQ)


def route_kernel(routes, up_far, send, order, up, sem):
    load = pltpu.make_async_copy(up_far.at[0], up, sem)
    load.start()
    send[...] = expand(places(routes, None)).astype(BF16)
    n = GRP * 128
    col = iota((n, n), 1)
    source = ((col >> 5) & 3) * 128 + (col >> 7) * 32 + (col & 31)
    order[...] = (iota((n, n), 0) == source).astype(F32).astype(BF16)
    load.wait()


def mix_kernel(place, m0, m1, m2, m3, tokens, mix_gain, ffn_gain, send, order, resid1, ffn_in, outgoing, pieces):
    for i, m in enumerate((m0, m1, m2, m3)):
        pieces[i] = m[...]
    own = place[0]
    got = [pieces[own ^ m] for m in range(GRP)]
    parts = []
    for i in range(COLS // 128):
        block = jnp.concatenate([g[:, i * 128 : (i + 1) * 128] for g in got], axis=1)
        parts.append(dot(block, order[...]))
    mixed = jnp.concatenate(parts, axis=1)
    r1 = tokens[...].astype(F32) + rms(mixed, mix_gain[...])
    resid1[...] = r1
    x = rms(r1, ffn_gain[...]).astype(BF16)
    ffn_in[...] = x
    blocks = jnp.concatenate([x[:, j * CH : (j + 1) * CH] for j in range(NJ)], axis=0)
    outgoing[...] = dot(send[...], blocks).astype(BF16)


def expert_kernel(incoming, gate, up, down, outgoing, rows, result, wd, back_rows, sems):
    copies = [pltpu.make_async_copy(down.at[0], wd, sems.at[0])]
    copies[0].start()
    n = 256
    a, b = iota((n, n), 0), iota((n, n), 1)
    order = (b == (a & 31) * NJ + (a >> 5)).astype(F32).astype(BF16)
    back = (a == (b & 31) * NJ + (b >> 5)).astype(F32).astype(BF16)
    for g in range(EP * 16 // n):
        block = dot(order, incoming[g * n : (g + 1) * n, :]).astype(BF16)
        for j in range(NJ):
            rows[g * 32 : (g + 1) * 32, j * CH : (j + 1) * CH] = block[j * 32 : (j + 1) * 32]
    x = rows[...]
    hidden = (jax.nn.silu(dot(x, gate[0])) * dot(x, up[...])).astype(BF16)
    copies[0].wait()
    result[...] = dot(hidden, wd[...]).astype(BF16)
    for g in range(EP * 16 // n):
        block = jnp.concatenate(
            [result[g * 32 : (g + 1) * 32, j * CH : (j + 1) * CH] for j in range(NJ)], axis=0
        )
        span = pl.ds(g * n, n)
        back_rows[span, :] = dot(back, block).astype(BF16)
        out = pltpu.make_async_copy(back_rows.at[span], outgoing.at[span], sems.at[1 + g])
        out.start()
        copies.append(out)
    for c in copies[1:]:
        c.wait()


def shared_kernel(x, tokens, routes, weights, mix_far, *refs):
    far, (out, high, low, nk, nv), (gain, wk, wv, gate, up, down, sems) = refs[:5], refs[5:10], refs[10:]
    copies = fetch((mix_far, *far), (gain, wk, wv, gate, up, down), sems)
    for c in copies[:3]:
        c.wait()
    mine = rms(tokens[...].astype(F32), gain[...]).astype(BF16)
    nk[...] = dot(mine, wk[...]).astype(BF16)
    nv[...] = dot(mine, wv[...]).astype(BF16)
    copies[3].wait()
    gated = jax.nn.silu(dot(x[...], gate[...]))
    copies[4].wait()
    hidden = (gated * dot(x[...], up[...])).astype(BF16)
    copies[5].wait()
    out[...] = dot(hidden, down[...])
    scaled = expand(places(routes, weights))
    top = scaled.astype(BF16)
    high[...] = top.T
    low[...] = (scaled - top.astype(F32)).astype(BF16).T


def final_kernel(returned, high, low, resid1, shared, gain, out):
    got = returned[...]
    total = dot(high[...], got) + dot(low[...], got)
    routed = jnp.concatenate([total[j * SEQ : (j + 1) * SEQ] for j in range(NJ)], axis=1)
    out[...] = (resid1[...] + rms(routed + shared[...], gain[...])).astype(BF16)


def call(kernel, ins, outs, smem=0, hbm=0, scratch=()):
    return pl.pallas_call(
        kernel,
        in_specs=[SMEM] * smem + [VMEM] * (ins - smem - hbm) + [HBM] * hbm,
        out_specs=[VMEM] * len(outs),
        out_shape=[jax.ShapeDtypeStruct(s, d) for s, d in outs],
        scratch_shapes=list(scratch),
        compiler_params=PARAMS,
    )


def in_hbm(x):
    return pltpu.with_memory_space_constraint(x, pltpu.HBM)


def swap(x, d):
    return lax.ppermute(x, "ep", [(i, i ^ d) for i in range(EP)])


def share(x):
    return [x] + [swap(x, XS * d) for d in range(1, GRP)]


def trade(parts):
    return [parts[0]] + [swap(parts[d], XS * d) for d in range(1, GRP)]


def gather_columns(weight):
    line = EP // PLANE
    groups = [[g + line * i for i in range(PLANE)] for g in range(line)]
    copies = jnp.broadcast_to(weight.T[None], (PLANE, SHARD, D))
    return lax.all_to_all(copies, "ep", 0, 0, tiled=True, axis_index_groups=groups)


def body(
    tokens, lengths, cache_keys, cache_values, mix_gain, mix_out_gain, ffn_gain, ffn_out_gain,
    query_weight, key_weight, value_weight, head_bias, output_weight, routes, route_weights,
    expert_gate, expert_up, expert_down, shared_gate, shared_up, shared_down,
):
    here = lax.axis_index("ep")
    place = jnp.stack([here // XS % GRP, here % 2]).astype(jnp.int32)
    group_tokens = share(tokens)
    own_q = gather_columns(query_weight)
    own_o = gather_columns(output_weight)
    route_rows = jnp.tile(routes.T, (1, NJ))
    weight_rows = jnp.tile(route_weights.T, (1, NJ))
    others = swap(jnp.concatenate(group_tokens, axis=0), 1)
    (rows,) = call(norm_kernel, 6, [((2 * GRP * SEQ, D), BF16)])(
        *group_tokens, others, mix_gain[None]
    )
    piece = ((SEQ, COLS), BF16)
    mine, others = call(query_kernel, 2, [((GRP * SEQ, COLS // 2), BF16)] * 2)(rows, own_q)
    got = swap(others, 1)
    queries = call(join_kernel, 2, [piece] * GRP)(mine, got)
    queries = trade(queries)
    attended = attend(
        place, lengths, queries, head_bias[:, None], cache_keys, cache_values
    )
    other_o = swap(own_o, 1)

    attended = share(attended)
    mixed = call(output_kernel, 7, [piece] * GRP, smem=1)(place, *attended, own_o, other_o)
    send, order, up = call(
        route_kernel, 2,
        [((EP * 16, NJ * SEQ), BF16), ((COLS, COLS), BF16), ((D, FF), BF16)],
        hbm=1, scratch=[pltpu.SemaphoreType.DMA],
    )(route_rows, in_hbm(expert_up))
    mixed = trade(mixed)
    resid1, ffn_in, outgoing = call(
        mix_kernel, 10,
        [((SEQ, D), F32), ((SEQ, D), BF16), ((EP * 16, CH), BF16)],
        smem=1, scratch=[pltpu.VMEM((GRP, SEQ, COLS), BF16)],
    )(place, *mixed, tokens, mix_out_gain[None], ffn_gain[None], send, order)

    incoming = lax.all_to_all(outgoing.reshape(EP, 16, CH), "ep", 0, 0, tiled=True)
    result = pl.pallas_call(
        expert_kernel,
        in_specs=[VMEM, VMEM, VMEM, HBM],
        out_specs=HBM,
        out_shape=jax.ShapeDtypeStruct((EP * 16, CH), BF16),
        scratch_shapes=[
            pltpu.VMEM((EP * CAP, D), BF16),
            pltpu.VMEM((EP * CAP, D), BF16),
            pltpu.VMEM((FF, D), BF16),
            pltpu.VMEM((EP * 16, CH), BF16),
            pltpu.SemaphoreType.DMA((9,)),
        ],
        compiler_params=PARAMS,
        name="expert",
    )(incoming.reshape(EP * 16, CH), expert_gate, up, in_hbm(expert_down))
    returned = lax.all_to_all(result.reshape(EP, 16, CH), "ep", 0, 0, tiled=True)
    shared_out, high, low, new_keys, new_values = pl.pallas_call(
        shared_kernel,
        in_specs=[VMEM] * 4 + [HBM] * 6,
        out_specs=[VMEM] * 5,
        out_shape=[jax.ShapeDtypeStruct((SEQ, D), F32)]
        + [jax.ShapeDtypeStruct((NJ * SEQ, EP * 16), BF16)] * 2
        + [jax.ShapeDtypeStruct((SEQ, 2 * HD), BF16)] * 2,
        scratch_shapes=[
            pltpu.VMEM((1, D), F32),
            pltpu.VMEM((D, 2 * HD), BF16),
            pltpu.VMEM((D, 2 * HD), BF16),
            pltpu.VMEM((D, FF), BF16),
            pltpu.VMEM((D, FF), BF16),
            pltpu.VMEM((FF, D), BF16),
            pltpu.SemaphoreType.DMA((6,)),
        ],
        compiler_params=PARAMS,
        name="shared",
    )(
        ffn_in, tokens, route_rows, weight_rows, in_hbm(mix_gain[None]), in_hbm(key_weight), in_hbm(value_weight),
        in_hbm(shared_gate), in_hbm(shared_up), in_hbm(shared_down),
    )
    (layer_out,) = call(final_kernel, 6, [((SEQ, D), BF16)])(
        returned.reshape(EP * 16, CH), high, low, resid1, shared_out,
        ffn_out_gain[None],
    )
    return (layer_out, new_keys, new_values)


def solution(mesh):
    row, full = P("ep", None), P()
    cube, col = P("ep", None, None), P(None, "ep")
    in_specs = (
        row, P("ep"), cube, cube, full, full, full, full, col, full, full, full, col, row, row,
        cube, cube, cube, full, full, full,
    )

    return jax.shard_map(body, mesh=mesh, in_specs=in_specs, out_specs=(row, row, row), check_vma=False)
```

```python
import jax
import jax.numpy as jnp
from jax import lax
from jax.experimental import pallas as pl
from jax.experimental.pallas import tpu as pltpu
from jax.sharding import PartitionSpec as P


D = 2048
HD = 64
H = 32
FF = 512
TOP = 6
SEQ = 16
LEN = 1024
EP = 128
GRP = 4
XS = 2
PLANE = 16
COLS = D // GRP
SHARD = D // EP
CAP = 2
CH = CAP * D // 16
NJ = D // CH
EPS = 1e-06
F32 = jnp.float32
BF16 = jnp.bfloat16

VMEM = pl.BlockSpec(memory_space=pltpu.VMEM)
HBM = pl.BlockSpec(memory_space=pltpu.HBM)
SMEM = pl.BlockSpec(memory_space=pltpu.SMEM)
PARAMS = pltpu.CompilerParams(vmem_limit_bytes=40 * 1024 * 1024)


def rms(rows, gain):
    return rows * lax.rsqrt(jnp.mean(rows * rows, axis=-1, keepdims=True) + EPS) * gain


def iota(shape, dim):
    return lax.broadcasted_iota(jnp.int32, shape, dim)


def dot(a, b):
    return jnp.dot(a, b, preferred_element_type=F32)


def dot_nt(a, b):
    return lax.dot_general(a, b, (((1,), (1,)), ((), ())), preferred_element_type=F32)


def project(place, rows, own, other, outs):
    for core in range(2):

        @pl.when(place[1] == core)
        def _():
            pair = (own, other) if core == 0 else (other, own)
            weight = jnp.concatenate([pair[c][p] for p in range(PLANE) for c in range(2)], axis=0)
            out = dot_nt(rows, weight).astype(BF16)
            for i, o in enumerate(outs):
                o[...] = out[i * SEQ : (i + 1) * SEQ]


def fetch(sources, targets, sems):
    copies = [pltpu.make_async_copy(s, t, sems.at[i]) for i, (s, t) in enumerate(zip(sources, targets))]
    for c in copies:
        c.start()
    return copies


def norm_kernel(t0, t1, t2, t3, others, gain, rows):
    for i, t in enumerate((t0, t1, t2, t3)):
        rows[i * SEQ : (i + 1) * SEQ] = rms(t[...].astype(F32), gain[...]).astype(BF16)
    rows[GRP * SEQ :] = rms(others[...].astype(F32), gain[...]).astype(BF16)


def query_kernel(rows, own, mine, others):
    weight = jnp.concatenate([own[p] for p in range(PLANE)], axis=0)
    out = dot_nt(rows[...], weight).astype(BF16)
    mine[...] = out[: GRP * SEQ]
    others[...] = out[GRP * SEQ :]


def join_kernel(mine, got, *outs):
    for i, o in enumerate(outs):
        o[...] = jnp.concatenate([mine[i * SEQ : (i + 1) * SEQ], got[i * SEQ : (i + 1) * SEQ]], axis=1)


SUB = 8
BLK = 256


def attend_kernel(place, lens, q0, q1, q2, q3, bias, keys, values, out, qf, placed, upper, att, kbuf, vbuf, sems):
    copies = []
    for g in range(SEQ // SUB):
        part = pl.ds(g * SUB, SUB)
        copies.append(
            [
                pltpu.make_async_copy(keys.at[part], kbuf.at[part], sems.at[0, g]),
                pltpu.make_async_copy(values.at[part], vbuf.at[part], sems.at[1, g]),
            ]
        )
    for c in copies[0]:
        c.start()

    upper[...] = (iota((BLK, BLK), 0) > iota((BLK, BLK), 1)).astype(F32).astype(BF16)
    for i, q in enumerate((q0, q1, q2, q3)):
        qf[i] = q[...].astype(F32) * HD ** (-0.5)
    row, col = iota((COLS, 2 * HD), 0), iota((COLS, 2 * HD), 1)
    plane, shard = (row >> 4) & (PLANE - 1), ((row >> 8) ^ place[1]) * SHARD + (row & 15)
    head = ((iota((H, COLS), 1) >> 4) & (PLANE - 1)) * 2
    spread = [[] for _ in range(SEQ)]
    select = []
    for m in range(GRP):
        target = (plane >> 3) * HD + (m & 1) * 32 + shard
        select.append((col == target).astype(F32).astype(BF16))
        mask = head + (m >> 1) == iota((H, COLS), 0)
        part = qf[(m - place[0]) & (GRP - 1)]
        for u in range(SEQ):
            rows = jnp.broadcast_to(part[u : u + 1], (H, COLS))
            spread[u].append(jnp.where(mask, rows, 0.0).astype(BF16))
    spread = jnp.concatenate([jnp.concatenate(p, axis=1) for p in spread], axis=0)
    placed[...] = dot(spread, jnp.concatenate(select, axis=0)).astype(BF16)

    count = LEN // BLK
    for g in range(SEQ // SUB):
        copies[g][0].wait()
        for c in copies[g + 1] if g + 1 < SEQ // SUB else ():
            c.start()
        valid, beta, keep, stacked = [], [], [], []
        for u in range(SUB):
            s = g * SUB + u
            z = dot_nt(placed[s * H : (s + 1) * H], kbuf[s]) + bias[...]
            valid.append(iota((H, LEN), 1) < lens[s])
            soft = jnp.log(1.0 + jnp.exp(-jnp.abs(z)))
            beta.append(jnp.minimum(z, 0.0) - soft)
            keep.append(jnp.where(valid[u], beta[u] - z, 0.0))
            high = keep[u].astype(BF16)
            low = (keep[u] - high.astype(F32)).astype(BF16)
            for b in range(count):
                stacked += [high[:, b * BLK : (b + 1) * BLK], low[:, b * BLK : (b + 1) * BLK]]
        later = dot(jnp.concatenate(stacked, axis=0), upper[...])
        copies[g][1].wait()
        for u in range(SUB):
            s = g * SUB + u
            carry = jnp.zeros((H, 1), F32)
            blocks = []
            for b in range(count - 1, -1, -1):
                at = (u * count + b) * 2 * H
                after = later[at : at + H] + later[at + H : at + 2 * H]
                blocks.append(after + carry)
                carry = carry + after[:, :1] + keep[u][:, b * BLK : b * BLK + 1]
            after = jnp.concatenate(blocks[::-1], axis=1)
            weights = jnp.where(valid[u], jnp.exp(beta[u] + after), 0.0).astype(BF16)
            att[s * H : (s + 1) * H, :] = dot(weights, vbuf[s])

    left = iota((SEQ, 2 * HD), 1) < HD
    for i in range(H // 2):
        even = att[pl.ds(2 * i, SEQ, stride=H), :]
        odd = att[pl.ds(2 * i + 1, SEQ, stride=H), :]
        if 2 * i < H // 2:
            odd = pltpu.roll(odd, HD, 1)
        else:
            even = pltpu.roll(even, HD, 1)
        out[:, i * 2 * HD : (i + 1) * 2 * HD] = jnp.where(left, even, odd).astype(BF16)


def attend(place, lengths, queries, bias, keys, values):
    return pl.pallas_call(
        attend_kernel,
        in_specs=[SMEM, SMEM] + [VMEM] * (GRP + 1) + [HBM, HBM],
        out_specs=VMEM,
        out_shape=jax.ShapeDtypeStruct((SEQ, D), BF16),
        scratch_shapes=[
            pltpu.VMEM((GRP, SEQ, COLS), F32),
            pltpu.VMEM((SEQ * H, 2 * HD), BF16),
            pltpu.VMEM((BLK, BLK), BF16),
            pltpu.VMEM((SEQ * H, 2 * HD), F32),
            pltpu.VMEM((SEQ, LEN, 2 * HD), BF16),
            pltpu.VMEM((SEQ, LEN, 2 * HD), BF16),
            pltpu.SemaphoreType.DMA((2, SEQ // SUB)),
        ],
        compiler_params=PARAMS,
        name="attend",
    )(place, lengths, *queries, bias, in_hbm(keys), in_hbm(values))


def output_kernel(place, a0, a1, a2, a3, own, other, *outs):
    rows = jnp.concatenate([a[...] for a in (a0, a1, a2, a3)], axis=0)
    project(place, rows, own, other, outs)


def places(routes, weights):
    shape = (EP * CAP, NJ * SEQ)
    row = iota(shape, 0)
    named = jnp.zeros(shape, F32)
    weight = jnp.zeros(shape, F32)
    for k in range(TOP):
        hit = jnp.broadcast_to(routes[k : k + 1, :], shape) == row >> 1
        named = named + hit.astype(F32)
        if weights is not None:
            weight = weight + jnp.where(hit, jnp.broadcast_to(weights[k : k + 1, :], shape), 0.0)
    a, b = iota((NJ * SEQ, NJ * SEQ), 0), iota((NJ * SEQ, NJ * SEQ), 1)
    earlier = (((a >> 4) == (b >> 4)) & (a < b)).astype(F32).astype(BF16)
    rank = dot(named.astype(BF16), earlier)
    here = jnp.where((rank == (row & 1).astype(F32)) & (named > 0.0), 1.0, 0.0)
    return here if weights is None else here * weight


def expand(x):
    block = (iota((NJ, NJ * SEQ), 0) == (iota((NJ, NJ * SEQ), 1) >> 4)).astype(F32)
    return (x[:, None, :] * block[None, :, :]).reshape(EP * CAP * NJ, NJ * SEQ)


def route_kernel(routes, up_far, send, order, up, sem):
    load = pltpu.make_async_copy(up_far.at[0], up, sem)
    load.start()
    send[...] = expand(places(routes, None)).astype(BF16)
    n = GRP * 128
    col = iota((n, n), 1)
    source = ((col >> 5) & 3) * 128 + (col >> 7) * 32 + (col & 31)
    order[...] = (iota((n, n), 0) == source).astype(F32).astype(BF16)
    load.wait()


def mix_kernel(place, m0, m1, m2, m3, tokens, mix_gain, ffn_gain, send, order, resid1, ffn_in, outgoing, pieces):
    for i, m in enumerate((m0, m1, m2, m3)):
        pieces[i] = m[...]
    own = place[0]
    got = [pieces[(m - own) & (GRP - 1)] for m in range(GRP)]
    parts = []
    for i in range(COLS // 128):
        block = jnp.concatenate([g[:, i * 128 : (i + 1) * 128] for g in got], axis=1)
        parts.append(dot(block, order[...]))
    mixed = jnp.concatenate(parts, axis=1)
    r1 = tokens[...].astype(F32) + rms(mixed, mix_gain[...])
    resid1[...] = r1
    x = rms(r1, ffn_gain[...]).astype(BF16)
    ffn_in[...] = x
    blocks = jnp.concatenate([x[:, j * CH : (j + 1) * CH] for j in range(NJ)], axis=0)
    outgoing[...] = dot(send[...], blocks).astype(BF16)


def expert_kernel(incoming, gate, up, down, outgoing, rows, result, wd, back_rows, sems):
    copies = [pltpu.make_async_copy(down.at[0], wd, sems.at[0])]
    copies[0].start()
    n = 256
    a, b = iota((n, n), 0), iota((n, n), 1)
    order = (b == (a & 31) * NJ + (a >> 5)).astype(F32).astype(BF16)
    back = (a == (b & 31) * NJ + (b >> 5)).astype(F32).astype(BF16)
    for g in range(EP * 16 // n):
        block = dot(order, incoming[g * n : (g + 1) * n, :]).astype(BF16)
        for j in range(NJ):
            rows[g * 32 : (g + 1) * 32, j * CH : (j + 1) * CH] = block[j * 32 : (j + 1) * 32]
    x = rows[...]
    hidden = (jax.nn.silu(dot(x, gate[0])) * dot(x, up[...])).astype(BF16)
    copies[0].wait()
    result[...] = dot(hidden, wd[...]).astype(BF16)
    for g in range(EP * 16 // n):
        block = jnp.concatenate(
            [result[g * 32 : (g + 1) * 32, j * CH : (j + 1) * CH] for j in range(NJ)], axis=0
        )
        span = pl.ds(g * n, n)
        back_rows[span, :] = dot(back, block).astype(BF16)
        out = pltpu.make_async_copy(back_rows.at[span], outgoing.at[span], sems.at[1 + g])
        out.start()
        copies.append(out)
    for c in copies[1:]:
        c.wait()


def shared_kernel(x, tokens, routes, weights, mix_far, *refs):
    far, (out, high, low, nk, nv), (gain, wk, wv, gate, up, down, sems) = refs[:5], refs[5:10], refs[10:]
    copies = fetch((mix_far, *far), (gain, wk, wv, gate, up, down), sems)
    for c in copies[:3]:
        c.wait()
    mine = rms(tokens[...].astype(F32), gain[...]).astype(BF16)
    nk[...] = dot(mine, wk[...]).astype(BF16)
    nv[...] = dot(mine, wv[...]).astype(BF16)
    copies[3].wait()
    gated = jax.nn.silu(dot(x[...], gate[...]))
    copies[4].wait()
    hidden = (gated * dot(x[...], up[...])).astype(BF16)
    copies[5].wait()
    out[...] = dot(hidden, down[...])
    scaled = expand(places(routes, weights))
    top = scaled.astype(BF16)
    high[...] = top.T
    low[...] = (scaled - top.astype(F32)).astype(BF16).T


def final_kernel(returned, high, low, resid1, shared, gain, out):
    got = returned[...]
    total = dot(high[...], got) + dot(low[...], got)
    routed = jnp.concatenate([total[j * SEQ : (j + 1) * SEQ] for j in range(NJ)], axis=1)
    out[...] = (resid1[...] + rms(routed + shared[...], gain[...])).astype(BF16)


def call(kernel, ins, outs, smem=0, hbm=0, scratch=()):
    return pl.pallas_call(
        kernel,
        in_specs=[SMEM] * smem + [VMEM] * (ins - smem - hbm) + [HBM] * hbm,
        out_specs=[VMEM] * len(outs),
        out_shape=[jax.ShapeDtypeStruct(s, d) for s, d in outs],
        scratch_shapes=list(scratch),
        compiler_params=PARAMS,
    )


def in_hbm(x):
    return pltpu.with_memory_space_constraint(x, pltpu.HBM)


def swap(x, d):
    return lax.ppermute(x, "ep", [(i, i ^ d) for i in range(EP)])


def shift(x, d):
    return lax.ppermute(
        x, "ep", [(i, i // 8 * 8 + (i // XS + d) % GRP * XS + i % 2) for i in range(EP)]
    )


def share(x):
    return [x] + [shift(x, d) for d in range(1, GRP)]


def trade(parts):
    return [parts[0]] + [shift(parts[d], -d) for d in range(1, GRP)]


def gather_columns(weight):
    line = EP // PLANE
    groups = [[g + line * i for i in range(PLANE)] for g in range(line)]
    copies = jnp.broadcast_to(weight.T[None], (PLANE, SHARD, D))
    return lax.all_to_all(copies, "ep", 0, 0, tiled=True, axis_index_groups=groups)


def body(
    tokens, lengths, cache_keys, cache_values, mix_gain, mix_out_gain, ffn_gain, ffn_out_gain,
    query_weight, key_weight, value_weight, head_bias, output_weight, routes, route_weights,
    expert_gate, expert_up, expert_down, shared_gate, shared_up, shared_down,
):
    here = lax.axis_index("ep")
    place = jnp.stack([here // XS % GRP, here % 2]).astype(jnp.int32)
    group_tokens = share(tokens)
    own_q = gather_columns(query_weight)
    own_o = gather_columns(output_weight)
    route_rows = jnp.tile(routes.T, (1, NJ))
    weight_rows = jnp.tile(route_weights.T, (1, NJ))
    others = swap(jnp.concatenate(group_tokens, axis=0), 1)
    (rows,) = call(norm_kernel, 6, [((2 * GRP * SEQ, D), BF16)])(
        *group_tokens, others, mix_gain[None]
    )
    piece = ((SEQ, COLS), BF16)
    mine, others = call(query_kernel, 2, [((GRP * SEQ, COLS // 2), BF16)] * 2)(rows, own_q)
    got = swap(others, 1)
    queries = call(join_kernel, 2, [piece] * GRP)(mine, got)
    queries = trade(queries)
    attended = attend(
        place, lengths, queries, head_bias[:, None], cache_keys, cache_values
    )
    other_o = swap(own_o, 1)

    attended = share(attended)
    mixed = call(output_kernel, 7, [piece] * GRP, smem=1)(place, *attended, own_o, other_o)
    send, order, up = call(
        route_kernel, 2,
        [((EP * 16, NJ * SEQ), BF16), ((COLS, COLS), BF16), ((D, FF), BF16)],
        hbm=1, scratch=[pltpu.SemaphoreType.DMA],
    )(route_rows, in_hbm(expert_up))
    mixed = trade(mixed)
    resid1, ffn_in, outgoing = call(
        mix_kernel, 10,
        [((SEQ, D), F32), ((SEQ, D), BF16), ((EP * 16, CH), BF16)],
        smem=1, scratch=[pltpu.VMEM((GRP, SEQ, COLS), BF16)],
    )(place, *mixed, tokens, mix_out_gain[None], ffn_gain[None], send, order)

    incoming = lax.all_to_all(outgoing.reshape(EP, 16, CH), "ep", 0, 0, tiled=True)
    result = pl.pallas_call(
        expert_kernel,
        in_specs=[VMEM, VMEM, VMEM, HBM],
        out_specs=HBM,
        out_shape=jax.ShapeDtypeStruct((EP * 16, CH), BF16),
        scratch_shapes=[
            pltpu.VMEM((EP * CAP, D), BF16),
            pltpu.VMEM((EP * CAP, D), BF16),
            pltpu.VMEM((FF, D), BF16),
            pltpu.VMEM((EP * 16, CH), BF16),
            pltpu.SemaphoreType.DMA((9,)),
        ],
        compiler_params=PARAMS,
        name="expert",
    )(incoming.reshape(EP * 16, CH), expert_gate, up, in_hbm(expert_down))
    returned = lax.all_to_all(result.reshape(EP, 16, CH), "ep", 0, 0, tiled=True)
    shared_out, high, low, new_keys, new_values = pl.pallas_call(
        shared_kernel,
        in_specs=[VMEM] * 4 + [HBM] * 6,
        out_specs=[VMEM] * 5,
        out_shape=[jax.ShapeDtypeStruct((SEQ, D), F32)]
        + [jax.ShapeDtypeStruct((NJ * SEQ, EP * 16), BF16)] * 2
        + [jax.ShapeDtypeStruct((SEQ, 2 * HD), BF16)] * 2,
        scratch_shapes=[
            pltpu.VMEM((1, D), F32),
            pltpu.VMEM((D, 2 * HD), BF16),
            pltpu.VMEM((D, 2 * HD), BF16),
            pltpu.VMEM((D, FF), BF16),
            pltpu.VMEM((D, FF), BF16),
            pltpu.VMEM((FF, D), BF16),
            pltpu.SemaphoreType.DMA((6,)),
        ],
        compiler_params=PARAMS,
        name="shared",
    )(
        ffn_in, tokens, route_rows, weight_rows, in_hbm(mix_gain[None]), in_hbm(key_weight), in_hbm(value_weight),
        in_hbm(shared_gate), in_hbm(shared_up), in_hbm(shared_down),
    )
    (layer_out,) = call(final_kernel, 6, [((SEQ, D), BF16)])(
        returned.reshape(EP * 16, CH), high, low, resid1, shared_out,
        ffn_out_gain[None],
    )
    return (layer_out, new_keys, new_values)


def solution(mesh):
    row, full = P("ep", None), P()
    cube, col = P("ep", None, None), P(None, "ep")
    in_specs = (
        row, P("ep"), cube, cube, full, full, full, full, col, full, full, full, col, row, row,
        cube, cube, cube, full, full, full,
    )

    return jax.shard_map(body, mesh=mesh, in_specs=in_specs, out_specs=(row, row, row), check_vma=False)
```

```python
import jax
import jax.numpy as jnp
from jax import lax
from jax.experimental import pallas as pl
from jax.experimental.pallas import tpu as pltpu
from jax.sharding import PartitionSpec as P


D = 2048
HD = 64
H = 32
FF = 512
TOP = 6
SEQ = 16
LEN = 1024
EP = 128
GRP = 4
XS = 2
PLANE = 16
COLS = D // GRP
SHARD = D // EP
CAP = 2
CH = CAP * D // 16
NJ = D // CH
EPS = 1e-06
F32 = jnp.float32
BF16 = jnp.bfloat16

VMEM = pl.BlockSpec(memory_space=pltpu.VMEM)
HBM = pl.BlockSpec(memory_space=pltpu.HBM)
SMEM = pl.BlockSpec(memory_space=pltpu.SMEM)
PARAMS = pltpu.CompilerParams(vmem_limit_bytes=40 * 1024 * 1024)


def rms(rows, gain):
    return rows * lax.rsqrt(jnp.mean(rows * rows, axis=-1, keepdims=True) + EPS) * gain


def iota(shape, dim):
    return lax.broadcasted_iota(jnp.int32, shape, dim)


def dot(a, b):
    return jnp.dot(a, b, preferred_element_type=F32)


def dot_nt(a, b):
    return lax.dot_general(a, b, (((1,), (1,)), ((), ())), preferred_element_type=F32)


def project(place, rows, own, other, outs):
    for core in range(2):

        @pl.when(place[1] == core)
        def _():
            pair = (own, other) if core == 0 else (other, own)
            weight = jnp.concatenate([pair[c][p] for p in range(PLANE) for c in range(2)], axis=0)
            out = dot_nt(rows, weight).astype(BF16)
            for i, o in enumerate(outs):
                o[...] = out[i * SEQ : (i + 1) * SEQ]


def fetch(sources, targets, sems):
    copies = [pltpu.make_async_copy(s, t, sems.at[i]) for i, (s, t) in enumerate(zip(sources, targets))]
    for c in copies:
        c.start()
    return copies


def norm_kernel(t0, t1, t2, t3, others, gain, rows):
    for i, t in enumerate((t0, t1, t2, t3)):
        rows[i * SEQ : (i + 1) * SEQ] = rms(t[...].astype(F32), gain[...]).astype(BF16)
    rows[GRP * SEQ :] = rms(others[...].astype(F32), gain[...]).astype(BF16)


def query_kernel(rows, own, mine, others):
    weight = jnp.concatenate([own[p] for p in range(PLANE)], axis=0)
    out = dot_nt(rows[...], weight).astype(BF16)
    mine[...] = out[: GRP * SEQ]
    others[...] = out[GRP * SEQ :]


def join_kernel(mine, got, *outs):
    for i, o in enumerate(outs):
        o[...] = jnp.concatenate([mine[i * SEQ : (i + 1) * SEQ], got[i * SEQ : (i + 1) * SEQ]], axis=1)


SUB = 8
BLK = 256


def attend_kernel(place, lens, q0, q1, q2, q3, bias, keys, values, out, qf, placed, upper, att, kbuf, vbuf, sems):
    copies = []
    for g in range(SEQ // SUB):
        part = pl.ds(g * SUB, SUB)
        copies.append(
            [
                pltpu.make_async_copy(keys.at[part], kbuf.at[part], sems.at[0, g]),
                pltpu.make_async_copy(values.at[part], vbuf.at[part], sems.at[1, g]),
            ]
        )
    for c in copies[0]:
        c.start()

    upper[...] = (iota((BLK, BLK), 0) > iota((BLK, BLK), 1)).astype(F32).astype(BF16)
    for i, q in enumerate((q0, q1, q2, q3)):
        qf[i] = q[...].astype(F32) * HD ** (-0.5)
    row, col = iota((COLS, 2 * HD), 0), iota((COLS, 2 * HD), 1)
    plane, shard = (row >> 4) & (PLANE - 1), ((row >> 8) ^ place[1]) * SHARD + (row & 15)
    head = ((iota((H, COLS), 1) >> 4) & (PLANE - 1)) * 2
    spread = [[] for _ in range(SEQ)]
    select = []
    for m in range(GRP):
        target = (plane >> 3) * HD + (m & 1) * 32 + shard
        select.append((col == target).astype(F32).astype(BF16))
        mask = head + (m >> 1) == iota((H, COLS), 0)
        part = qf[(m - place[0]) & (GRP - 1)]
        for u in range(SEQ):
            rows = jnp.broadcast_to(part[u : u + 1], (H, COLS))
            spread[u].append(jnp.where(mask, rows, 0.0).astype(BF16))
    spread = jnp.concatenate([jnp.concatenate(p, axis=1) for p in spread], axis=0)
    placed[...] = dot(spread, jnp.concatenate(select, axis=0)).astype(BF16)

    count = LEN // BLK
    for g in range(SEQ // SUB):
        copies[g][0].wait()
        for c in copies[g + 1] if g + 1 < SEQ // SUB else ():
            c.start()
        valid, beta, keep, stacked = [], [], [], []
        for u in range(SUB):
            s = g * SUB + u
            z = dot_nt(placed[s * H : (s + 1) * H], kbuf[s]) + bias[...]
            valid.append(iota((H, LEN), 1) < lens[s])
            soft = jnp.log(1.0 + jnp.exp(-jnp.abs(z)))
            beta.append(jnp.minimum(z, 0.0) - soft)
            keep.append(jnp.where(valid[u], beta[u] - z, 0.0))
            high = keep[u].astype(BF16)
            low = (keep[u] - high.astype(F32)).astype(BF16)
            for b in range(count):
                stacked += [high[:, b * BLK : (b + 1) * BLK], low[:, b * BLK : (b + 1) * BLK]]
        later = dot(jnp.concatenate(stacked, axis=0), upper[...])
        copies[g][1].wait()
        for u in range(SUB):
            s = g * SUB + u
            carry = jnp.zeros((H, 1), F32)
            blocks = []
            for b in range(count - 1, -1, -1):
                at = (u * count + b) * 2 * H
                after = later[at : at + H] + later[at + H : at + 2 * H]
                blocks.append(after + carry)
                carry = carry + after[:, :1] + keep[u][:, b * BLK : b * BLK + 1]
            after = jnp.concatenate(blocks[::-1], axis=1)
            weights = jnp.where(valid[u], jnp.exp(beta[u] + after), 0.0).astype(BF16)
            att[s * H : (s + 1) * H, :] = dot(weights, vbuf[s])

    left = iota((SEQ, 2 * HD), 1) < HD
    for i in range(H // 2):
        even = att[pl.ds(2 * i, SEQ, stride=H), :]
        odd = att[pl.ds(2 * i + 1, SEQ, stride=H), :]
        if 2 * i < H // 2:
            odd = pltpu.roll(odd, HD, 1)
        else:
            even = pltpu.roll(even, HD, 1)
        out[:, i * 2 * HD : (i + 1) * 2 * HD] = jnp.where(left, even, odd).astype(BF16)


def attend(place, lengths, queries, bias, keys, values):
    return pl.pallas_call(
        attend_kernel,
        in_specs=[SMEM, SMEM] + [VMEM] * (GRP + 1) + [HBM, HBM],
        out_specs=VMEM,
        out_shape=jax.ShapeDtypeStruct((SEQ, D), BF16),
        scratch_shapes=[
            pltpu.VMEM((GRP, SEQ, COLS), F32),
            pltpu.VMEM((SEQ * H, 2 * HD), BF16),
            pltpu.VMEM((BLK, BLK), BF16),
            pltpu.VMEM((SEQ * H, 2 * HD), F32),
            pltpu.VMEM((SEQ, LEN, 2 * HD), BF16),
            pltpu.VMEM((SEQ, LEN, 2 * HD), BF16),
            pltpu.SemaphoreType.DMA((2, SEQ // SUB)),
        ],
        compiler_params=PARAMS,
        name="attend",
    )(place, lengths, *queries, bias, in_hbm(keys), in_hbm(values))


def output_kernel(place, a0, a1, a2, a3, own, other, *outs):
    rows = jnp.concatenate([a[...] for a in (a0, a1, a2, a3)], axis=0)
    project(place, rows, own, other, outs)


def places(routes, weights):
    shape = (EP * CAP, NJ * SEQ)
    row = iota(shape, 0)
    named = jnp.zeros(shape, F32)
    weight = jnp.zeros(shape, F32)
    for k in range(TOP):
        hit = jnp.broadcast_to(routes[k : k + 1, :], shape) == row >> 1
        named = named + hit.astype(F32)
        if weights is not None:
            weight = weight + jnp.where(hit, jnp.broadcast_to(weights[k : k + 1, :], shape), 0.0)
    a, b = iota((NJ * SEQ, NJ * SEQ), 0), iota((NJ * SEQ, NJ * SEQ), 1)
    earlier = (((a >> 4) == (b >> 4)) & (a < b)).astype(F32).astype(BF16)
    rank = dot(named.astype(BF16), earlier)
    here = jnp.where((rank == (row & 1).astype(F32)) & (named > 0.0), 1.0, 0.0)
    return here if weights is None else here * weight


def expand(x):
    block = (iota((NJ, NJ * SEQ), 0) == (iota((NJ, NJ * SEQ), 1) >> 4)).astype(F32)
    return (x[:, None, :] * block[None, :, :]).reshape(EP * CAP * NJ, NJ * SEQ)


def route_kernel(routes, up_far, send, order, up, sem):
    load = pltpu.make_async_copy(up_far.at[0], up, sem)
    load.start()
    send[...] = expand(places(routes, None)).astype(BF16)
    n = GRP * 128
    col = iota((n, n), 1)
    source = ((col >> 5) & 3) * 128 + (col >> 7) * 32 + (col & 31)
    order[...] = (iota((n, n), 0) == source).astype(F32).astype(BF16)
    load.wait()


def mix_kernel(place, m0, m1, m2, m3, tokens, mix_gain, ffn_gain, send, order, resid1, ffn_in, outgoing, pieces):
    for i, m in enumerate((m0, m1, m2, m3)):
        pieces[i] = m[...]
    own = place[0]
    got = [pieces[(m - own) & (GRP - 1)] for m in range(GRP)]
    parts = []
    for i in range(COLS // 128):
        block = jnp.concatenate([g[:, i * 128 : (i + 1) * 128] for g in got], axis=1)
        parts.append(dot(block, order[...]))
    mixed = jnp.concatenate(parts, axis=1)
    r1 = tokens[...].astype(F32) + rms(mixed, mix_gain[...])
    resid1[...] = r1
    x = rms(r1, ffn_gain[...]).astype(BF16)
    ffn_in[...] = x
    blocks = jnp.concatenate([x[:, j * CH : (j + 1) * CH] for j in range(NJ)], axis=0)
    outgoing[...] = dot(send[...], blocks).astype(BF16)


def expert_kernel(incoming, gate, up, down, outgoing, rows, result, wd, back_rows, sems):
    copies = [pltpu.make_async_copy(down.at[0], wd, sems.at[0])]
    copies[0].start()
    n = 256
    a, b = iota((n, n), 0), iota((n, n), 1)
    order = (b == (a & 31) * NJ + (a >> 5)).astype(F32).astype(BF16)
    back = (a == (b & 31) * NJ + (b >> 5)).astype(F32).astype(BF16)
    for g in range(EP * 16 // n):
        block = dot(order, incoming[g * n : (g + 1) * n, :]).astype(BF16)
        for j in range(NJ):
            rows[g * 32 : (g + 1) * 32, j * CH : (j + 1) * CH] = block[j * 32 : (j + 1) * 32]
    x = rows[...]
    hidden = (jax.nn.silu(dot(x, gate[0])) * dot(x, up[...])).astype(BF16)
    copies[0].wait()
    result[...] = dot(hidden, wd[...]).astype(BF16)
    for g in range(EP * 16 // n):
        block = jnp.concatenate(
            [result[g * 32 : (g + 1) * 32, j * CH : (j + 1) * CH] for j in range(NJ)], axis=0
        )
        span = pl.ds(g * n, n)
        back_rows[span, :] = dot(back, block).astype(BF16)
        out = pltpu.make_async_copy(back_rows.at[span], outgoing.at[span], sems.at[1 + g])
        out.start()
        copies.append(out)
    for c in copies[1:]:
        c.wait()


def shared_kernel(x, tokens, routes, weights, mix_far, *refs):
    far, (out, high, low, nk, nv), (gain, wk, wv, gate, up, down, sems) = refs[:5], refs[5:10], refs[10:]
    copies = fetch((mix_far, *far), (gain, wk, wv, gate, up, down), sems)
    for c in copies[:3]:
        c.wait()
    mine = rms(tokens[...].astype(F32), gain[...]).astype(BF16)
    nk[...] = dot(mine, wk[...]).astype(BF16)
    nv[...] = dot(mine, wv[...]).astype(BF16)
    copies[3].wait()
    gated = jax.nn.silu(dot(x[...], gate[...]))
    copies[4].wait()
    hidden = (gated * dot(x[...], up[...])).astype(BF16)
    copies[5].wait()
    out[...] = dot(hidden, down[...])
    scaled = expand(places(routes, weights))
    top = scaled.astype(BF16)
    high[...] = top.T
    low[...] = (scaled - top.astype(F32)).astype(BF16).T


def final_kernel(returned, high, low, resid1, shared, gain, out):
    got = returned[...]
    total = dot(high[...], got) + dot(low[...], got)
    routed = jnp.concatenate([total[j * SEQ : (j + 1) * SEQ] for j in range(NJ)], axis=1)
    out[...] = (resid1[...] + rms(routed + shared[...], gain[...])).astype(BF16)


def call(kernel, ins, outs, smem=0, hbm=0, scratch=()):
    return pl.pallas_call(
        kernel,
        in_specs=[SMEM] * smem + [VMEM] * (ins - smem - hbm) + [HBM] * hbm,
        out_specs=[VMEM] * len(outs),
        out_shape=[jax.ShapeDtypeStruct(s, d) for s, d in outs],
        scratch_shapes=list(scratch),
        compiler_params=PARAMS,
    )


def in_hbm(x):
    return pltpu.with_memory_space_constraint(x, pltpu.HBM)


def swap(x, d):
    return lax.ppermute(x, "ep", [(i, i ^ d) for i in range(EP)])


def shift(x, d):
    return lax.ppermute(x, "ep", [(i, i // 8 * 8 + (i // XS + d) % GRP * XS + i % 2) for i in range(EP)])


FAR_FIRST = (2, 1, 3)


def share(x):
    got = {d: shift(x, d) for d in FAR_FIRST}
    return [x] + [got[d] for d in range(1, GRP)]


def trade(parts):
    got = {d: shift(parts[d], -d) for d in FAR_FIRST}
    return [parts[0]] + [got[d] for d in range(1, GRP)]


def gather_columns(weight):
    line = EP // PLANE
    groups = [[g + line * i for i in range(PLANE)] for g in range(line)]
    copies = jnp.broadcast_to(weight.T[None], (PLANE, SHARD, D))
    return lax.all_to_all(copies, "ep", 0, 0, tiled=True, axis_index_groups=groups)


def body(
    tokens, lengths, cache_keys, cache_values, mix_gain, mix_out_gain, ffn_gain, ffn_out_gain,
    query_weight, key_weight, value_weight, head_bias, output_weight, routes, route_weights,
    expert_gate, expert_up, expert_down, shared_gate, shared_up, shared_down,
):
    here = lax.axis_index("ep")
    place = jnp.stack([here // XS % GRP, here % 2]).astype(jnp.int32)
    group_tokens = share(tokens)
    own_q = gather_columns(query_weight)
    own_o = gather_columns(output_weight)
    route_rows = jnp.tile(routes.T, (1, NJ))
    weight_rows = jnp.tile(route_weights.T, (1, NJ))
    others = swap(jnp.concatenate(group_tokens, axis=0), 1)
    (rows,) = call(norm_kernel, 6, [((2 * GRP * SEQ, D), BF16)])(
        *group_tokens, others, mix_gain[None]
    )
    piece = ((SEQ, COLS), BF16)
    mine, others = call(query_kernel, 2, [((GRP * SEQ, COLS // 2), BF16)] * 2)(rows, own_q)
    got = swap(others, 1)
    queries = call(join_kernel, 2, [piece] * GRP)(mine, got)
    queries = trade(queries)
    attended = attend(
        place, lengths, queries, head_bias[:, None], cache_keys, cache_values
    )
    other_o = swap(own_o, 1)

    attended = share(attended)
    mixed = call(output_kernel, 7, [piece] * GRP, smem=1)(place, *attended, own_o, other_o)
    send, order, up = call(
        route_kernel, 2,
        [((EP * 16, NJ * SEQ), BF16), ((COLS, COLS), BF16), ((D, FF), BF16)],
        hbm=1, scratch=[pltpu.SemaphoreType.DMA],
    )(route_rows, in_hbm(expert_up))
    mixed = trade(mixed)
    resid1, ffn_in, outgoing = call(
        mix_kernel, 10,
        [((SEQ, D), F32), ((SEQ, D), BF16), ((EP * 16, CH), BF16)],
        smem=1, scratch=[pltpu.VMEM((GRP, SEQ, COLS), BF16)],
    )(place, *mixed, tokens, mix_out_gain[None], ffn_gain[None], send, order)

    incoming = lax.all_to_all(outgoing.reshape(EP, 16, CH), "ep", 0, 0, tiled=True)
    result = pl.pallas_call(
        expert_kernel,
        in_specs=[VMEM, VMEM, VMEM, HBM],
        out_specs=HBM,
        out_shape=jax.ShapeDtypeStruct((EP * 16, CH), BF16),
        scratch_shapes=[
            pltpu.VMEM((EP * CAP, D), BF16),
            pltpu.VMEM((EP * CAP, D), BF16),
            pltpu.VMEM((FF, D), BF16),
            pltpu.VMEM((EP * 16, CH), BF16),
            pltpu.SemaphoreType.DMA((9,)),
        ],
        compiler_params=PARAMS,
        name="expert",
    )(incoming.reshape(EP * 16, CH), expert_gate, up, in_hbm(expert_down))
    returned = lax.all_to_all(result.reshape(EP, 16, CH), "ep", 0, 0, tiled=True)
    shared_out, high, low, new_keys, new_values = pl.pallas_call(
        shared_kernel,
        in_specs=[VMEM] * 4 + [HBM] * 6,
        out_specs=[VMEM] * 5,
        out_shape=[jax.ShapeDtypeStruct((SEQ, D), F32)]
        + [jax.ShapeDtypeStruct((NJ * SEQ, EP * 16), BF16)] * 2
        + [jax.ShapeDtypeStruct((SEQ, 2 * HD), BF16)] * 2,
        scratch_shapes=[
            pltpu.VMEM((1, D), F32),
            pltpu.VMEM((D, 2 * HD), BF16),
            pltpu.VMEM((D, 2 * HD), BF16),
            pltpu.VMEM((D, FF), BF16),
            pltpu.VMEM((D, FF), BF16),
            pltpu.VMEM((FF, D), BF16),
            pltpu.SemaphoreType.DMA((6,)),
        ],
        compiler_params=PARAMS,
        name="shared",
    )(
        ffn_in, tokens, route_rows, weight_rows, in_hbm(mix_gain[None]), in_hbm(key_weight), in_hbm(value_weight),
        in_hbm(shared_gate), in_hbm(shared_up), in_hbm(shared_down),
    )
    (layer_out,) = call(final_kernel, 6, [((SEQ, D), BF16)])(
        returned.reshape(EP * 16, CH), high, low, resid1, shared_out,
        ffn_out_gain[None],
    )
    return (layer_out, new_keys, new_values)


def solution(mesh):
    row, full = P("ep", None), P()
    cube, col = P("ep", None, None), P(None, "ep")
    in_specs = (
        row, P("ep"), cube, cube, full, full, full, full, col, full, full, full, col, row, row,
        cube, cube, cube, full, full, full,
    )

    return jax.shard_map(body, mesh=mesh, in_specs=in_specs, out_specs=(row, row, row), check_vma=False)
```
